256 devices in a mesh: sp: 64 (over z, y, core), tp: 4 (over x).
Axes of the slice: x: 4, y: 4, z: 8, core: 2. Of those that a mesh axis runs over, the one named last changes fastest.
Arguments:
- query_one: bfloat16 [16384, 512], P('sp', 'tp'), may hold values from -190 to 190
- query_two: bfloat16 [16384, 512], P('sp', 'tp'), may hold values from -190 to 190
- key_one: bfloat16 [16384, 512], P('sp', 'tp'), may hold values from -10 to 10
- key_two: bfloat16 [16384, 512], P('sp', 'tp'), may hold values from -10 to 10
- values: bfloat16 [16384, 1024], P('sp', 'tp'), may hold values from -6 to 6
- mix_lambda: float32 [8], P('tp'), may hold values from 0.3 to 0.8
- head_gain: float32 [128], replicated, may hold values from 0.1 to 1.9
- stream: bfloat16 [16384, 2048], P('sp', 'tp'), may hold values from -6 to 6
- out_weight: bfloat16 [1024, 2048], P('tp'), may hold values from -0.1875 to 0.1875
- first_gain: float32 [2048], replicated, may hold values from 0.1 to 1.9
- up_weight: bfloat16 [2048, 4096], P('sp', 'tp'), may hold values from -0.125 to 0.125
- down_weight: bfloat16 [4096, 2048], P('tp', 'sp'), may hold values from -0.09375 to 0.09375
- second_gain: float32 [2048], replicated, may hold values from 0.1 to 1.9
Outputs:
- layer_out: bfloat16 [16384, 2048], P(('sp', 'tp'))
The draws below stay inside these ranges and needn't reach their ends.
All inputs are finite; a program needn't handle non-finite values.
Results may differ from the reference program's by a relative error of at most 0.019.
Values may be sent and summed in bfloat16 or wider, within the bound.
A program may use at most 128 MiB of HBM per device.

```python
import math
import jax
import jax.numpy as jnp
from jax import lax

D = 2048
HEADS = 8
QK = 64
VD = 128
FF = 4096
SEQ = 16384
HV = 1024


def drawn_pair(key, which):
    key_query = jax.random.fold_in(key, 11 + which)
    key_keys = jax.random.fold_in(key, 23 + which)
    width = HEADS * QK
    keys_drawn = jnp.clip(jax.random.normal(key_keys, (SEQ, width), jnp.float32), -7.0, 7.0) * 1.3
    queries = jnp.clip(jax.random.normal(key_query, (SEQ, width), jnp.float32), -7.0, 7.0) * 1.3
    return (queries, keys_drawn)


def draw_query_one(key, part):
    return drawn_pair(key, 1)[0].astype(jnp.bfloat16)


def draw_key_one(key, part):
    return drawn_pair(key, 1)[1].astype(jnp.bfloat16)


def draw_query_two(key, part):
    return drawn_pair(key, 2)[0].astype(jnp.bfloat16)


def draw_key_two(key, part):
    return drawn_pair(key, 2)[1].astype(jnp.bfloat16)


def block_scale(rng, dims, split, low, high):
    level, own = 1.0, jax.random.fold_in(rng, 6)
    for dim, blocks in split:
        heights = jnp.exp(jax.random.uniform(jax.random.fold_in(own, dim), (blocks,), jnp.float32, low / len(split), high / len(split)))
        level = level * jnp.repeat(heights, dims[dim] // blocks).reshape([-1 if axis == dim else 1 for axis in range(len(dims))])
    return level


def noise(stream_key, shape, scale, reach, cuts=(), held_as=jnp.bfloat16):
    result = scale * jax.random.normal(stream_key, shape, jnp.float32)
    if cuts:
        result = result * block_scale(stream_key, shape, cuts, -0.22, 0.18)
    return jnp.clip(result, -reach, reach).astype(held_as)


def setup_inputs(seed: int = 0) -> dict:
    key_of = jax.random.split(jax.random.key(seed), 14)
    query_one = draw_query_one(jax.random.fold_in(key_of[13], 71), 0)
    query_two = draw_query_two(jax.random.fold_in(key_of[13], 71), 0)
    key_one = draw_key_one(jax.random.fold_in(key_of[13], 71), 0)
    key_two = draw_key_two(jax.random.fold_in(key_of[13], 71), 0)
    values = noise(key_of[4], (SEQ, HV), 1.0, 6.0, ((0, 64), (1, 4)))
    mix_lambda = jnp.clip(0.3 + 0.5 * jax.random.uniform(key_of[5], (HEADS,), jnp.float32) ** block_scale(key_of[5], (HEADS,), ((0, 4),), -0.2, 0.2), 0.3, 0.8)
    head_gain = jnp.clip(1.0 + 0.18 * jax.random.normal(key_of[6], (VD,), jnp.float32), 0.1, 1.9)
    stream = noise(key_of[7], (SEQ, D), 1.0, 6.0, ((0, 64), (1, 4)))
    out_weight = noise(key_of[8], (HV, D), HV ** -0.5, 0.1875, ((0, 4),))
    first_gain = jnp.clip(1.0 + 0.18 * jax.random.normal(key_of[9], (D,), jnp.float32), 0.1, 1.9)
    up_weight = noise(key_of[10], (D, FF), D ** -0.5, 0.125, ((0, 64), (1, 4)))
    down_weight = noise(key_of[11], (FF, D), FF ** -0.5, 0.09375, ((0, 4), (1, 64)))
    second_gain = jnp.clip(1.0 + 0.18 * jax.random.normal(key_of[12], (D,), jnp.float32), 0.1, 1.9)
    return dict(query_one=query_one, query_two=query_two, key_one=key_one, key_two=key_two, values=values, mix_lambda=mix_lambda, head_gain=head_gain, stream=stream, out_weight=out_weight, first_gain=first_gain, up_weight=up_weight, down_weight=down_weight, second_gain=second_gain)


alpha_mix = 2.0 ** 0.5

def layer_norm(value, gain):
    centre = lax.optimization_barrier(jnp.mean(value, axis=-1, keepdims=True))
    spread = lax.optimization_barrier(jnp.mean(jnp.square(value - centre), axis=-1, keepdims=True))
    return (value - centre) * lax.rsqrt(spread + 1e-05) * gain

def one_map(query_blk, keys, values):
    scores = jnp.dot(query_blk, keys.T, preferred_element_type=jnp.float32) * QK ** (-0.5)
    shifted = scores - lax.optimization_barrier(jnp.max(scores, axis=-1, keepdims=True))
    expo = jnp.exp(shifted)
    total = lax.optimization_barrier(jnp.sum(expo, axis=-1, keepdims=True))
    return jnp.dot(expo.astype(jnp.bfloat16), values, preferred_element_type=jnp.float32) / total

def reference(query_one, query_two, key_one, key_two, values, mix_lambda, head_gain, stream, out_weight, first_gain, up_weight, down_weight, second_gain):

    def heads(array, width):
        return jnp.transpose(array.reshape(SEQ, HEADS, width), (1, 0, 2))
    qblk = math.gcd(SEQ, 512)
    nblk = SEQ // qblk

    def per_head(args):
        q_one, q_two, k_one, k_two, vals, weight = args
        q_one = q_one.reshape(nblk, qblk, QK)
        q_two = q_two.reshape(nblk, qblk, QK)

        def per_block(pair):
            return one_map(pair[0], k_one, vals) - weight * one_map(pair[1], k_two, vals)
        return lax.map(per_block, (q_one, q_two)).reshape(SEQ, VD)
    mixed = lax.map(per_head, (heads(query_one, QK), heads(query_two, QK), heads(key_one, QK), heads(key_two, QK), heads(values, VD), mix_lambda))
    normed = mixed * lax.rsqrt(lax.optimization_barrier(jnp.mean(jnp.square(mixed), axis=-1, keepdims=True)) + 1e-05) * head_gain * 0.8
    attended = jnp.transpose(normed.astype(jnp.bfloat16), (1, 0, 2)).reshape(SEQ, HV)
    pre = alpha_mix * stream.astype(jnp.float32) + jnp.dot(attended, out_weight, preferred_element_type=jnp.float32)
    hidden_in = layer_norm(pre, first_gain).astype(jnp.bfloat16)
    upper = jnp.dot(hidden_in, up_weight, preferred_element_type=jnp.float32)
    act = jnp.square(jax.nn.relu(upper)).astype(jnp.bfloat16)
    post = alpha_mix * hidden_in.astype(jnp.float32) + jnp.dot(act, down_weight, preferred_element_type=jnp.float32)
    return layer_norm(post, second_gain).astype(jnp.bfloat16)
```

```python
import functools

import jax
import jax.numpy as jnp
from jax import lax
from jax.experimental import pallas as pl
from jax.experimental.pallas import tpu as pltpu
from jax.sharding import PartitionSpec as P

MESH = pl.DeviceIdType.MESH
NZ, NY, NX = 8, 4, 4
ALPHA = 2.0**0.5
LOG2E = 1.4426950408889634
CEXP = LOG2E * 64 ** (-0.5)
LOW = -1e30
TOK = 256
SUB = 64
NT = (((1,), (1,)), ((), ()))


def layer_norm(value, gain):
    centre = jnp.mean(value, axis=-1, keepdims=True)
    spread = jnp.mean(jnp.square(value - centre), axis=-1, keepdims=True)
    return (value - centre) * lax.rsqrt(spread + 1e-05) * gain


def attention_kernel(
    lam_ref, q1_ref, q2_ref, k1_ref, k2_ref, v_ref, gain_ref, stream_ref,
    att_out, str_out,
    kvsrc, qsrc, kvbuf, qbuf, acc, mbuf, lbuf, osend, ssend, orecv, srecv, attown, attbuf, strbuf,
    snd, kv_rcv, q_rcv, o_rcv, s_rcv, str_rcv, att_rcv,
):
    sp = lax.axis_index("sp")
    x = lax.axis_index("tp")
    c = lax.rem(sp, 2)
    y = lax.rem(sp // 2, NY)
    z = sp // (2 * NY)

    def dev(dz=0, dy=0, core=None, dx=0):
        zz = lax.rem(z + (dz + NZ), NZ)
        yy = lax.rem(y + (dy + NY), NY)
        cc = c if core is None else core
        return {"sp": (zz * NY + yy) * 2 + cc, "tp": lax.rem(x + (dx + NX), NX)}

    count = [0]
    started = []

    def send(src, dst, rcv, to):
        k = count[0]
        count[0] += 1
        cp = pltpu.make_async_remote_copy(
            src_ref=src, dst_ref=dst, send_sem=snd.at[k], recv_sem=rcv, device_id=to, device_id_type=MESH
        )
        cp.start()
        started.append(cp)

    def arrived(dst, rcv):
        pltpu.make_async_remote_copy(
            src_ref=dst, dst_ref=dst, send_sem=snd.at[0], recv_sem=rcv, device_id=dev(core=1 - c),
            device_id_type=MESH,
        ).wait_recv()

    barrier = pltpu.get_barrier_semaphore()
    partners = [dev(core=1 - c), dev(dy=2)]
    for core in (0, 1):
        partners += [dev(dz=1, core=core), dev(dz=-1, core=core), dev(dy=1, core=core), dev(dy=-1, core=core)]
        partners += [dev(dx=d, core=core) for d in (1, 2, 3)]
    for p in partners:
        pl.semaphore_signal(barrier, inc=1, device_id=p, device_id_type=MESH)

    lane = lax.broadcasted_iota(jnp.int32, (TOK, 128), 1)
    low_half = lane < 64

    def by_head(one_ref, two_ref):
        one, two = one_ref[...].astype(jnp.float32), two_ref[...].astype(jnp.float32)
        first = jnp.where(low_half, one, pltpu.roll(two, 64, 1))
        second = jnp.where(low_half, pltpu.roll(one, 64, 1), two)
        return first.astype(jnp.bfloat16), second.astype(jnp.bfloat16)

    for h, part in enumerate(by_head(q1_ref, q2_ref)):
        qsrc[h] = part
    vt = v_ref[...].astype(jnp.float32).T.astype(jnp.bfloat16)
    for h, part in enumerate(by_head(k1_ref, k2_ref)):
        kvsrc[h, 0:256, :] = part
        kvsrc[h, 256:384, :] = vt[128 * h : 128 * h + 128, 0:128]
        kvsrc[h, 384:512, :] = vt[128 * h : 128 * h + 128, 128:256]
    kvbuf[0, c] = kvsrc[c]
    qbuf[0, c] = qsrc[c]
    strbuf[x] = stream_ref[pl.ds(pl.multiple_of(x * SUB, SUB), SUB), :]
    mbuf[...] = jnp.full(mbuf.shape, LOW, jnp.float32)
    lbuf[...] = jnp.zeros(lbuf.shape, jnp.float32)

    def clear(i, carry):
        acc[i] = jnp.zeros(acc.shape[1:], jnp.float32)
        return carry

    lax.fori_loop(0, acc.shape[0], clear, 0)
    pl.semaphore_wait(barrier, len(partners))

    sibling = dev(core=1 - c)
    send(qsrc.at[1 - c], qbuf.at[0, c], q_rcv.at[0, c], sibling)
    send(kvsrc.at[1 - c], kvbuf.at[0, c], kv_rcv.at[0, c], sibling)
    for h in (0, 1):
        send(kvsrc.at[h], kvbuf.at[1, c], kv_rcv.at[1, c], dev(dz=1, core=h))
        send(kvsrc.at[h], kvbuf.at[2, c], kv_rcv.at[2, c], dev(dz=-1, core=h))
        send(qsrc.at[h], qbuf.at[1, c], q_rcv.at[1, c], dev(dy=1, core=h))
        send(qsrc.at[h], qbuf.at[2, c], q_rcv.at[2, c], dev(dy=-1, core=h))
    for dx in (1, 2, 3):
        rows = pl.ds(pl.multiple_of(lax.rem(x + dx, NX) * SUB, SUB), SUB)
        send(stream_ref.at[rows, :], strbuf.at[x], str_rcv.at[dx - 1], dev(dx=dx))

    def take_kv(slot):
        for cc in (0, 1):
            arrived(kvbuf.at[slot, cc], kv_rcv.at[slot, cc])
            step = 1 if slot % 2 else -1
            if slot <= 4:
                send(kvbuf.at[slot, cc], kvbuf.at[slot + 2, cc], kv_rcv.at[slot + 2, cc], dev(dz=step))
            elif (slot, cc) in ((5, 0), (6, 1)):
                send(kvbuf.at[slot, cc], kvbuf.at[7, cc], kv_rcv.at[7, cc], dev(dz=step))

    def take_q(slot):
        for cc in (0, 1):
            arrived(qbuf.at[slot, cc], q_rcv.at[slot, cc])
            if (slot, cc) in ((1, 0), (2, 1)):
                send(qbuf.at[slot, cc], qbuf.at[3, cc], q_rcv.at[3, cc], dev(dy=1 if slot == 1 else -1))

    row_lane = lax.broadcasted_iota(jnp.int32, (1, 128), 1)
    masks = [jnp.where(row_lane < 64, 1.0, 0.0).astype(jnp.bfloat16), jnp.where(row_lane < 64, 0.0, 1.0).astype(jnp.bfloat16)]

    def unit(kvs, qs):
        keys = jnp.concatenate([kvbuf[kvs, cc, 0:256, :] for cc in (0, 1)], axis=0)
        vals = jnp.concatenate(
            [kvbuf[kvs, cc, 256 + 128 * i : 384 + 128 * i, :] for cc in (0, 1) for i in (0, 1)], axis=1
        )
        for cc in (0, 1):
            for mp in (0, 1):
                at = qs * 4 + (2 * cc + mp)
                query = qbuf[qs, cc] * masks[mp]
                scores = lax.dot_general(keys, query, NT, preferred_element_type=jnp.float32)
                old = mbuf[at]
                new = jnp.maximum(old, jnp.max(scores, axis=0, keepdims=True))
                factor = jnp.exp2((old - new) * CEXP)
                expo = jnp.exp2((scores - new) * CEXP)
                mbuf[at] = new
                lbuf[at] = lbuf[at] * factor + jnp.sum(expo, axis=0, keepdims=True)
                acc[at] = acc[at] * factor + jnp.dot(
                    vals, expo.astype(jnp.bfloat16), preferred_element_type=jnp.float32
                )

    def process(kv_lo, kv_n, q_lo, q_n):
        def trip(i, carry):
            unit(kv_lo + i // q_n, q_lo + lax.rem(i, q_n))
            return carry

        lax.fori_loop(0, kv_n * q_n, trip, 0)

    def finish(qs):
        for cc in (0, 1):
            for mp in (0, 1):
                at = qs * 4 + 2 * cc + mp
                osend[qs - 1, 2 * cc + mp] = (acc[at] / lbuf[at]).astype(jnp.bfloat16)
        for cc in (0, 1):
            for mp in (0, 1):
                at = qs * 4 + 2 * cc + mp
                ssend[qs - 1, 2 * cc + mp] = mbuf[at]
                ssend[qs - 1, 4 + 2 * cc + mp] = lbuf[at]
        to, land = {1: (dev(dy=-1), 1), 2: (dev(dy=1), 0), 3: (dev(dy=2), 2)}[qs]
        send(osend.at[qs - 1], orecv.at[land], o_rcv.at[land], to)
        send(ssend.at[qs - 1], srecv.at[land], s_rcv.at[land], to)

    arrived(qbuf.at[0, 1 - c], q_rcv.at[0, 1 - c])
    arrived(kvbuf.at[0, 1 - c], kv_rcv.at[0, 1 - c])
    process(0, 1, 0, 1)
    take_q(1)
    take_q(2)
    process(0, 1, 1, 2)
    take_kv(1)
    take_kv(2)
    process(1, 2, 0, 3)
    take_q(3)
    process(0, 3, 3, 1)
    take_kv(3)
    take_kv(4)
    process(3, 2, 0, 4)
    take_kv(5)
    take_kv(6)
    take_kv(7)
    for qs in (3, 1, 2):
        process(5, 3, qs, 1)
        finish(qs)
    process(5, 3, 0, 1)

    for j in (2, 1, 0):
        arrived(orecv.at[j], o_rcv.at[j])
        arrived(srecv.at[j], s_rcv.at[j])
    lam = lam_ref[c]
    gain = gain_ref[...] * 0.8
    for cc in (0, 1):
        maps = []
        for mp in (0, 1):
            i = 2 * cc + mp
            ms = [mbuf[i]] + [srecv[j, i] for j in range(3)]
            ls = [lbuf[i]] + [srecv[j, 4 + i] for j in range(3)]
            top = functools.reduce(jnp.maximum, ms)
            ws = [jnp.exp2((m - top) * CEXP) for m in ms]
            total = ws[0] * ls[0]
            out = acc[i] * ws[0]
            for j in range(3):
                w = ws[j + 1] * ls[j + 1]
                total = total + w
                out = out + orecv[j, i].astype(jnp.float32) * w
            maps.append(out / total)
        mixed = maps[0] - lam * maps[1]
        inv = lax.rsqrt(jnp.mean(mixed * mixed, axis=0, keepdims=True) + 1e-5)
        attown[cc] = ((mixed * inv).T * gain).astype(jnp.bfloat16)

    head = 2 * x + c
    for dx in range(NX):
        for dc in (0, 1):
            if dx == 0 and dc == 0:
                continue
            cc = c if dc == 0 else 1 - c
            rows = pl.ds(pl.multiple_of(lax.rem(x + dx, NX) * SUB, SUB), SUB)
            send(attown.at[cc, rows, :], attbuf.at[head], att_rcv.at[2 * dx + dc - 1], dev(dx=dx, core=cc))
    attbuf[head] = attown[c, pl.ds(pl.multiple_of(x * SUB, SUB), SUB), :]
    for dx in (1, 2, 3):
        src = lax.rem(x + (NX - dx), NX)
        arrived(strbuf.at[src], str_rcv.at[dx - 1])
    for dx in range(NX):
        for dc in (0, 1):
            if dx == 0 and dc == 0:
                continue
            cc = c if dc == 0 else 1 - c
            src = 2 * lax.rem(x + (NX - dx), NX) + cc
            arrived(attbuf.at[src], att_rcv.at[2 * dx + dc - 1])
    for h in range(8):
        att_out[:, 128 * h : 128 * h + 128] = attbuf[h]
    for i in range(NX):
        str_out[:, 512 * i : 512 * i + 512] = strbuf[i]
    for cp in started:
        cp.wait_send()


def attention(lam, q1, q2, k1, k2, v, gain, stream):
    bf, f32 = jnp.bfloat16, jnp.float32
    vm = pl.BlockSpec(memory_space=pltpu.VMEM)
    dma = pltpu.SemaphoreType.DMA
    return pl.pallas_call(
        attention_kernel,
        out_shape=(jax.ShapeDtypeStruct((SUB, 1024), bf), jax.ShapeDtypeStruct((SUB, 2048), bf)),
        in_specs=[pl.BlockSpec(memory_space=pltpu.SMEM)] + [vm] * 7,
        out_specs=(vm, vm),
        scratch_shapes=[
            pltpu.VMEM((2, 512, 128), bf),
            pltpu.VMEM((2, 256, 128), bf),
            pltpu.VMEM((8, 2, 512, 128), bf),
            pltpu.VMEM((4, 2, 256, 128), bf),
            pltpu.VMEM((16, 128, 256), f32),
            pltpu.VMEM((16, 1, 256), f32),
            pltpu.VMEM((16, 1, 256), f32),
            pltpu.VMEM((3, 4, 128, 256), bf),
            pltpu.VMEM((3, 8, 1, 256), f32),
            pltpu.VMEM((3, 4, 128, 256), bf),
            pltpu.VMEM((3, 8, 1, 256), f32),
            pltpu.VMEM((2, 256, 128), bf),
            pltpu.VMEM((8, SUB, 128), bf),
            pltpu.VMEM((NX, SUB, 512), bf),
            dma((48,)),
            dma((8, 2)),
            dma((4, 2)),
            dma((3,)),
            dma((3,)),
            dma((3,)),
            dma((7,)),
        ],
        compiler_params=pltpu.CompilerParams(
            collective_id=0, has_side_effects=True, vmem_limit_bytes=40 * 1024 * 1024
        ),
        cost_estimate=pl.CostEstimate(flops=20_000_000_000, bytes_accessed=4_000_000, transcendentals=17_000_000),
        name="attention",
    )(lam, q1, q2, k1, k2, v, gain.reshape(1, 128), stream)


def in_blocks(value, dim, size):
    shape = value.shape
    parts = value.reshape(*shape[:dim], size, shape[dim] // size, *shape[dim + 1 :])
    return jnp.moveaxis(parts, dim, 0)


def local(
    query_one, query_two, key_one, key_two, values, mix_lambda, head_gain, stream, out_weight, first_gain,
    up_weight, down_weight, second_gain,
):
    bf, f32 = jnp.bfloat16, jnp.float32
    both = jnp.concatenate([up_weight, down_weight.T], axis=0)
    weights = lax.all_gather(both, "sp", axis=0, tiled=False)
    up_full = weights[:, 0:32, :].reshape(2048, 1024)
    down_t = weights[:, 32:64, :].reshape(2048, 1024)
    out_full = lax.all_gather(out_weight, "tp", axis=0, tiled=True)
    attended, rows = attention(mix_lambda, query_one, query_two, key_one, key_two, values, head_gain, stream)
    pre = ALPHA * rows.astype(f32) + jnp.dot(attended, out_full, preferred_element_type=f32)
    own = layer_norm(pre, first_gain).astype(bf)
    hidden = lax.all_to_all(jnp.broadcast_to(own, (NX, *own.shape)), "tp", 0, 0, tiled=True).reshape(TOK, 2048)
    upper = jnp.dot(hidden, up_full, preferred_element_type=f32)
    act = jnp.square(jax.nn.relu(upper)).astype(bf)
    part = lax.dot_general(act, down_t, NT, preferred_element_type=f32).astype(bf)
    parts = lax.all_to_all(part.reshape(NX, SUB, 2048), "tp", 0, 0, tiled=True)
    post = jnp.sum(parts.astype(f32), axis=0) + ALPHA * own.astype(f32)
    return layer_norm(post, second_gain).astype(bf)


def solution(mesh):
    in_specs = (
        P("sp", "tp"), P("sp", "tp"), P("sp", "tp"), P("sp", "tp"), P("sp", "tp"), P("tp"), P(), P("sp", "tp"),
        P("tp", None), P(), P("sp", "tp"), P("tp", "sp"), P(),
    )
    return jax.shard_map(
        local, mesh=mesh, in_specs=in_specs, out_specs=P(("sp", "tp"), None), check_vma=False
    )
```

```python
import functools

import jax
import jax.numpy as jnp
from jax import lax
from jax.experimental import pallas as pl
from jax.experimental.pallas import tpu as pltpu
from jax.sharding import PartitionSpec as P

MESH = pl.DeviceIdType.MESH
NZ, NY, NX = 8, 4, 4
ALPHA = 2.0**0.5
LOG2E = 1.4426950408889634
CEXP = LOG2E * 64 ** (-0.5)
LOW = -1e30
TOK = 256
SUB = 64
NT = (((1,), (1,)), ((), ()))


def layer_norm(value, gain):
    centre = jnp.mean(value, axis=-1, keepdims=True)
    spread = jnp.mean(jnp.square(value - centre), axis=-1, keepdims=True)
    return (value - centre) * lax.rsqrt(spread + 1e-05) * gain


def layer_kernel(
    lam_ref, q1_hbm, q2_hbm, k1_hbm, k2_hbm, v_hbm, hgain_hbm, stream_hbm, ow_hbm, gain1_hbm, up_hbm, down_hbm, gain2_hbm,
    out_ref,
    q1_ref, q2_ref, k1_ref, k2_ref, v_ref, gain_ref, gain1_ref, gain2_ref,
    kvsrc, qsrc, kvbuf, qbuf, acc, mbuf, lbuf, qexp, sbuf, topbuf, osend, ssend, orecv, srecv, attown, attbuf, strbuf,
    wout, wup, wdn, hid, psend, precv, prelay,
    snd, loc, kv_rcv, q_rcv, o_rcv, s_rcv, str_rcv, att_rcv,
    upy_rcv, upz_rcv, updd_rcv, dnz_rcv, dny_rcv, dndd_rcv, ow_rcv, owdd_rcv, hid_rcv, p_rcv, pr_rcv,
):
    sp = lax.axis_index("sp")
    x = lax.axis_index("tp")
    c = lax.rem(sp, 2)
    y = lax.rem(sp // 2, NY)
    z = sp // (2 * NY)
    f = 1 - 2 * c

    def at_z(d):
        return lax.rem(z + (d + NZ), NZ)

    def at_y(d):
        return lax.rem(y + (d + NY), NY)

    def at_x(d):
        return lax.rem(x + (d + NX), NX)

    def dev(dz=0, dy=0, core=None, dx=0):
        cc = c if core is None else core
        return {"sp": (at_z(dz) * NY + at_y(dy)) * 2 + cc, "tp": at_x(dx)}

    sibling = dev(core=1 - c)
    started = []

    def send(src, dst, rcv, to):
        cp = pltpu.make_async_remote_copy(
            src_ref=src, dst_ref=dst, send_sem=snd.at[len(started)], recv_sem=rcv, device_id=to, device_id_type=MESH
        )
        cp.start()
        started.append(cp)

    def arrived(dst, rcv):
        pltpu.make_async_remote_copy(
            src_ref=dst, dst_ref=dst, send_sem=snd.at[0], recv_sem=rcv, device_id=sibling, device_id_type=MESH
        ).wait_recv()

    mine = pl.ds(pl.multiple_of(x * SUB, SUB), SUB)

    def ow_rows(d, half):
        return pl.ds(pl.multiple_of((2 * at_x(d) + half) * 128, 128), 128)

    local_pairs = [
        (q1_hbm, q1_ref), (q2_hbm, q2_ref), (k1_hbm, k1_ref), (k2_hbm, k2_ref), (v_hbm, v_ref),
        (hgain_hbm, gain_ref), (gain1_hbm, gain1_ref), (gain2_hbm, gain2_ref),
        (stream_hbm.at[mine, :], strbuf.at[x]),
        (up_hbm, wup.at[z, y, c]), (down_hbm, wdn.at[z, y, c]),
        (ow_hbm, wout.at[pl.ds(pl.multiple_of(x * 256, 256), 256), :]),
    ]
    locals_ = [pltpu.make_async_copy(a, b, loc.at[i]) for i, (a, b) in enumerate(local_pairs)]
    for cp in locals_:
        cp.start()

    barrier = pltpu.get_barrier_semaphore()
    partners = [sibling, dev(dy=2)]
    for core in (0, 1):
        partners += [dev(dz=1, core=core), dev(dz=-1, core=core), dev(dy=1, core=core), dev(dy=-1, core=core)]
        partners += [dev(dx=d, core=core) for d in (1, 2, 3)]
    for p in partners:
        pl.semaphore_signal(barrier, inc=1, device_id=p, device_id_type=MESH)

    mbuf[...] = jnp.full(mbuf.shape, LOW, jnp.float32)
    lbuf[...] = jnp.zeros(lbuf.shape, jnp.float32)

    def clear(i, carry):
        acc[i] = jnp.zeros(acc.shape[1:], jnp.float32)
        return carry

    lax.fori_loop(0, acc.shape[0], clear, 0)
    for cp in locals_[:5]:
        cp.wait()

    lane = lax.broadcasted_iota(jnp.int32, (TOK, 128), 1)
    low_half = lane < 64
    q1t = q1_ref[...].astype(jnp.float32).T.astype(jnp.bfloat16)
    q2t = q2_ref[...].astype(jnp.float32).T.astype(jnp.bfloat16)
    for h in (0, 1):
        qsrc[h, 0:64, :] = q1t[64 * h : 64 * h + 64]
        qsrc[h, 64:128, :] = q2t[64 * h : 64 * h + 64]
    vt = v_ref[...].astype(jnp.float32).T.astype(jnp.bfloat16)
    one, two = k1_ref[...].astype(jnp.float32), k2_ref[...].astype(jnp.float32)
    kvsrc[0, 0:256, :] = jnp.where(low_half, one, pltpu.roll(two, 64, 1)).astype(jnp.bfloat16)
    kvsrc[1, 0:256, :] = jnp.where(low_half, pltpu.roll(one, 64, 1), two).astype(jnp.bfloat16)
    for h in (0, 1):
        kvsrc[h, 256:384, :] = vt[128 * h : 128 * h + 128, 0:128]
        kvsrc[h, 384:512, :] = vt[128 * h : 128 * h + 128, 128:256]
    kvbuf[0, c] = kvsrc[c]
    qbuf[0, c] = qsrc[c]
    pl.semaphore_wait(barrier, len(partners))

    send(qsrc.at[1 - c], qbuf.at[0, c], q_rcv.at[0, c], sibling)
    send(kvsrc.at[1 - c], kvbuf.at[0, c], kv_rcv.at[0, c], sibling)
    for h in (0, 1):
        send(kvsrc.at[h], kvbuf.at[1, c], kv_rcv.at[1, c], dev(dz=1, core=h))
        send(kvsrc.at[h], kvbuf.at[2, c], kv_rcv.at[2, c], dev(dz=-1, core=h))
        send(qsrc.at[h], qbuf.at[1, c], q_rcv.at[1, c], dev(dy=1, core=h))
        send(qsrc.at[h], qbuf.at[2, c], q_rcv.at[2, c], dev(dy=-1, core=h))
    for dx in (1, 2, 3):
        rows = pl.ds(pl.multiple_of(at_x(dx) * SUB, SUB), SUB)
        send(stream_hbm.at[rows, :], strbuf.at[x], str_rcv.at[dx - 1], dev(dx=dx))
    half_rows = pl.ds(pl.multiple_of(c * 128, 128), 128)
    for i, d in enumerate((1, -1)):
        send(ow_hbm.at[half_rows, :], wout.at[ow_rows(0, c), :], ow_rcv.at[i], dev(dx=d))
        send(up_hbm, wup.at[z, y, c], upy_rcv.at[i], dev(dy=d))
        send(down_hbm, wdn.at[z, y, c], dnz_rcv.at[i], dev(dz=d))

    def out_weight_on():
        arrived(wout.at[ow_rows(-1, c), :], ow_rcv.at[0])
        arrived(wout.at[ow_rows(1, c), :], ow_rcv.at[1])
        blk = wout.at[ow_rows(-f, c), :]
        send(blk, blk, ow_rcv.at[2], dev(dx=f))
        for i, d in enumerate((-1, 1)):
            blk = wout.at[ow_rows(d, c), :]
            send(blk, blk, owdd_rcv.at[i], sibling)

    def out_weight_end():
        blk = wout.at[ow_rows(2, c), :]
        arrived(blk, ow_rcv.at[2])
        send(blk, blk, owdd_rcv.at[2], sibling)

    def up_y_on():
        arrived(wup.at[z, at_y(-1), c], upy_rcv.at[0])
        arrived(wup.at[z, at_y(1), c], upy_rcv.at[1])
        blk = wup.at[z, at_y(-f), c]
        send(blk, blk, upy_rcv.at[2], dev(dy=f))

    def up_y_end():
        arrived(wup.at[z, at_y(2), c], upy_rcv.at[2])
        locals_[9].wait()

    def up_z_start():
        blk = wup.at[z, :, c]
        for i, d in enumerate((1, -1)):
            send(blk, blk, upz_rcv.at[i], dev(dz=d))
        send(blk, blk, updd_rcv.at[0], sibling)

    def up_z_step(d):
        if d == 4:
            blk = wup.at[at_z(4), :, c]
            arrived(blk, upz_rcv.at[6])
            send(blk, blk, updd_rcv.at[7], sibling)
            return
        for i, s in enumerate((-1, 1)):
            blk = wup.at[at_z(s * d), :, c]
            arrived(blk, upz_rcv.at[2 * (d - 1) + i])
            if d < 3:
                send(blk, blk, upz_rcv.at[2 * d + i], dev(dz=-s))
        if d == 3:
            blk = wup.at[at_z(-3 * f), :, c]
            send(blk, blk, upz_rcv.at[6], dev(dz=f))
        for i, s in enumerate((-1, 1)):
            blk = wup.at[at_z(s * d), :, c]
            send(blk, blk, updd_rcv.at[2 * (d - 1) + 1 + i], sibling)

    def down_z_step(d):
        if d == 4:
            arrived(wdn.at[at_z(4), y, c], dnz_rcv.at[6])
            return
        for i, s in enumerate((-1, 1)):
            blk = wdn.at[at_z(s * d), y, c]
            arrived(blk, dnz_rcv.at[2 * (d - 1) + i])
            if d < 3:
                send(blk, blk, dnz_rcv.at[2 * d + i], dev(dz=-s))
        if d == 3:
            blk = wdn.at[at_z(-3 * f), y, c]
            send(blk, blk, dnz_rcv.at[6], dev(dz=f))

    def down_y_start():
        locals_[10].wait()
        blk = wdn.at[:, y, c]
        for i, d in enumerate((1, -1)):
            send(blk, blk, dny_rcv.at[i], dev(dy=d))
        send(blk, blk, dndd_rcv.at[0], sibling)

    def down_y_on():
        arrived(wdn.at[:, at_y(-1), c], dny_rcv.at[0])
        arrived(wdn.at[:, at_y(1), c], dny_rcv.at[1])
        blk = wdn.at[:, at_y(-f), c]
        send(blk, blk, dny_rcv.at[2], dev(dy=f))
        for i, d in enumerate((-1, 1)):
            blk = wdn.at[:, at_y(d), c]
            send(blk, blk, dndd_rcv.at[1 + i], sibling)

    def down_y_end():
        blk = wdn.at[:, at_y(2), c]
        arrived(blk, dny_rcv.at[2])
        send(blk, blk, dndd_rcv.at[3], sibling)

    def take_kv(slot):
        for cc in (0, 1):
            arrived(kvbuf.at[slot, cc], kv_rcv.at[slot, cc])
            step = 1 if slot % 2 else -1
            if slot <= 4:
                send(kvbuf.at[slot, cc], kvbuf.at[slot + 2, cc], kv_rcv.at[slot + 2, cc], dev(dz=step))
            elif (slot, cc) in ((5, 0), (6, 1)):
                send(kvbuf.at[slot, cc], kvbuf.at[7, cc], kv_rcv.at[7, cc], dev(dz=step))

    def take_q(slot):
        for cc in (0, 1):
            arrived(qbuf.at[slot, cc], q_rcv.at[slot, cc])
            if (slot, cc) in ((1, 0), (2, 1)):
                send(qbuf.at[slot, cc], qbuf.at[3, cc], q_rcv.at[3, cc], dev(dy=1 if slot == 1 else -1))

    def expand(qs):
        for cc in (0, 1):
            scaled = qbuf[qs, cc].astype(jnp.float32) * CEXP
            high = scaled.astype(jnp.bfloat16)
            rest = (scaled - high.astype(jnp.float32)).astype(jnp.bfloat16)
            blank = jnp.zeros((64, 256), jnp.bfloat16)
            for mp in (0, 1):
                own = slice(64 * mp, 64 * mp + 64)
                other = slice(64 - 64 * mp, 128 - 64 * mp)
                at = qs * 4 + 2 * cc + mp
                qexp[at, own, :] = high[own]
                qexp[at, other, :] = blank
                own = slice(128 + 64 * mp, 192 + 64 * mp)
                other = slice(192 - 64 * mp, 256 - 64 * mp)
                qexp[at, own, :] = rest[64 * mp : 64 * mp + 64]
                qexp[at, other, :] = blank

    def score(kvs, qs, j):
        slot = j % 4
        keys = jnp.concatenate([kvbuf[kvs, cc, 0:256, :] for cc in (0, 1)], axis=0)
        keys = jnp.concatenate([keys, keys], axis=1)
        scores = jnp.dot(keys, qexp[qs * 4 + j], preferred_element_type=jnp.float32)
        sbuf[slot] = scores
        topbuf[slot] = jnp.max(scores.reshape(64, 8, 256), axis=0)

    def absorb(kvs, qs, j):
        slot = j % 4
        at = qs * 4 + j
        vals = jnp.concatenate(
            [kvbuf[kvs, cc, 256 + 128 * i : 384 + 128 * i, :] for cc in (0, 1) for i in (0, 1)], axis=1
        )
        old = mbuf[at]
        new = jnp.maximum(old, jnp.max(topbuf[slot], axis=0, keepdims=True))
        factor = jnp.exp2(old - new)
        expo = jnp.exp2(sbuf[slot] - new)
        mbuf[at] = new
        lbuf[at] = lbuf[at] * factor + jnp.sum(expo, axis=0, keepdims=True)
        acc[at] = acc[at] * factor + jnp.dot(vals, expo.astype(jnp.bfloat16), preferred_element_type=jnp.float32)

    def process(kv_lo, kv_n, q_lo, q_n):
        last = kv_n * q_n - 1

        def place(i):
            return kv_lo + i // q_n, q_lo + lax.rem(i, q_n)

        def trip(i, carry):
            kvs, qs = place(i)
            nkvs, nqs = place(jnp.minimum(i + 1, last))
            for j in range(4):
                if j < 2:
                    score(kvs, qs, j + 2)
                else:
                    score(nkvs, nqs, j - 2)
                absorb(kvs, qs, j)
            return carry

        score(kv_lo, q_lo, 0)
        score(kv_lo, q_lo, 1)
        lax.fori_loop(0, last + 1, trip, 0)

    def finish(qs):
        for cc in (0, 1):
            for mp in (0, 1):
                at = qs * 4 + 2 * cc + mp
                osend[qs - 1, 2 * cc + mp] = (acc[at] / lbuf[at]).astype(jnp.bfloat16)
        for cc in (0, 1):
            for mp in (0, 1):
                at = qs * 4 + 2 * cc + mp
                ssend[qs - 1, 2 * cc + mp] = mbuf[at]
                ssend[qs - 1, 4 + 2 * cc + mp] = lbuf[at]
        to, land = {1: (dev(dy=-1), 1), 2: (dev(dy=1), 0), 3: (dev(dy=2), 2)}[qs]
        send(osend.at[qs - 1], orecv.at[land], o_rcv.at[land], to)
        send(ssend.at[qs - 1], srecv.at[land], s_rcv.at[land], to)

    arrived(qbuf.at[0, 1 - c], q_rcv.at[0, 1 - c])
    expand(0)
    arrived(kvbuf.at[0, 1 - c], kv_rcv.at[0, 1 - c])
    process(0, 1, 0, 1)
    take_q(1)
    take_q(2)
    expand(1)
    expand(2)
    process(0, 1, 1, 2)
    take_kv(1)
    take_kv(2)
    down_z_step(1)
    up_y_on()
    process(1, 2, 0, 3)
    take_q(3)
    expand(3)
    process(0, 3, 3, 1)
    take_kv(3)
    take_kv(4)
    down_z_step(2)
    out_weight_on()
    up_y_end()
    process(3, 2, 0, 4)
    take_kv(5)
    take_kv(6)
    down_z_step(3)
    up_z_start()
    take_kv(7)
    process(5, 3, 3, 1)
    finish(3)
    down_z_step(4)
    out_weight_end()
    process(5, 3, 1, 1)
    finish(1)
    process(5, 3, 2, 1)
    finish(2)
    down_y_start()
    up_z_step(1)
    process(5, 3, 0, 1)
    up_z_step(2)

    for j in (2, 1, 0):
        arrived(orecv.at[j], o_rcv.at[j])
        arrived(srecv.at[j], s_rcv.at[j])
    locals_[5].wait()
    lam = lam_ref[c]
    gain = gain_ref[...] * 0.8
    for cc in (0, 1):
        maps = []
        for mp in (0, 1):
            i = 2 * cc + mp
            ms = [mbuf[i]] + [srecv[j, i] for j in range(3)]
            ls = [lbuf[i]] + [srecv[j, 4 + i] for j in range(3)]
            top = functools.reduce(jnp.maximum, ms)
            ws = [jnp.exp2(m - top) for m in ms]
            total = ws[0] * ls[0]
            out = acc[i] * ws[0]
            for j in range(3):
                w = ws[j + 1] * ls[j + 1]
                total = total + w
                out = out + orecv[j, i].astype(jnp.float32) * w
            maps.append(out / total)
        mixed = maps[0] - lam * maps[1]
        inv = lax.rsqrt(jnp.mean(mixed * mixed, axis=0, keepdims=True) + 1e-5)
        attown[cc] = ((mixed * inv).T * gain).astype(jnp.bfloat16)


    head = 2 * x + c
    for dx in range(NX):
        for dc in (0, 1):
            if dx == 0 and dc == 0:
                continue
            cc = c if dc == 0 else 1 - c
            rows = pl.ds(pl.multiple_of(at_x(dx) * SUB, SUB), SUB)
            send(attown.at[cc, rows, :], attbuf.at[head], att_rcv.at[2 * dx + dc - 1], dev(dx=dx, core=cc))
    attbuf[head] = attown[c, mine, :]
    up_z_step(3)
    down_y_on()
    for i in range(3):
        arrived(wout.at[ow_rows((-1, 1, 2)[i], 1 - c), :], owdd_rcv.at[i])
    for i in (6, 7, 8, 11):
        locals_[i].wait()
    for dx in (1, 2, 3):
        arrived(strbuf.at[at_x(-dx)], str_rcv.at[dx - 1])
    for dx in range(NX):
        for dc in (0, 1):
            if dx == 0 and dc == 0:
                continue
            cc = c if dc == 0 else 1 - c
            arrived(attbuf.at[2 * at_x(-dx) + cc], att_rcv.at[2 * dx + dc - 1])
    attended = jnp.concatenate([attbuf[h] for h in range(8)], axis=1)
    rows = jnp.concatenate([strbuf[i] for i in range(NX)], axis=1).astype(jnp.float32)
    pre = ALPHA * rows + jnp.dot(attended, wout[...], preferred_element_type=jnp.float32)
    own = layer_norm(pre, gain1_ref[...]).astype(jnp.bfloat16)
    hid[x] = own
    up_z_step(4)
    for i, d in enumerate((1, -1)):
        send(hid.at[x], hid.at[x], hid_rcv.at[i], dev(dx=d))
    down_y_end()
    arrived(wup.at[z, :, 1 - c], updd_rcv.at[0])
    for d in (1, 2, 3):
        for i, s in enumerate((-1, 1)):
            arrived(wup.at[at_z(s * d), :, 1 - c], updd_rcv.at[2 * (d - 1) + 1 + i])
    arrived(wup.at[at_z(4), :, 1 - c], updd_rcv.at[7])
    arrived(wdn.at[:, y, 1 - c], dndd_rcv.at[0])
    for i, d in enumerate((-1, 1)):
        arrived(wdn.at[:, at_y(d), 1 - c], dndd_rcv.at[1 + i])
    arrived(wdn.at[:, at_y(2), 1 - c], dndd_rcv.at[3])

    def mixer(tokens):
        total = None
        for n in range(4):
            up = wup[:, :, :, :, 256 * n : 256 * n + 256].reshape(2048, 256)
            upper = jnp.dot(tokens, up, preferred_element_type=jnp.float32)
            act = jnp.square(jnp.maximum(upper, 0.0)).astype(jnp.bfloat16)
            down = wdn[:, :, :, :, 256 * n : 256 * n + 256].reshape(2048, 256)
            part = lax.dot_general(act, down, NT, preferred_element_type=jnp.float32)
            total = part if total is None else total + part
        return total

    post = mixer(own) + ALPHA * own.astype(jnp.float32)
    arrived(hid.at[at_x(-1)], hid_rcv.at[0])
    arrived(hid.at[at_x(1)], hid_rcv.at[1])
    send(hid.at[at_x(-f)], hid.at[at_x(-f)], hid_rcv.at[2], dev(dx=f))
    both = mixer(jnp.concatenate([hid[at_x(-1)], hid[at_x(1)]], axis=0)).astype(jnp.bfloat16)
    psend[0] = both[0:SUB]
    psend[1] = both[SUB:]
    send(psend.at[0], precv.at[1], p_rcv.at[1], dev(dx=-1))
    send(psend.at[1], precv.at[0], p_rcv.at[0], dev(dx=1))
    arrived(hid.at[at_x(2)], hid_rcv.at[2])
    psend[2] = mixer(hid[at_x(2)]).astype(jnp.bfloat16)
    send(psend.at[2], prelay, pr_rcv.at[0], dev(dx=f))
    arrived(prelay, pr_rcv.at[0])
    send(prelay, precv.at[2], p_rcv.at[2], dev(dx=f))
    for i in range(3):
        arrived(precv.at[i], p_rcv.at[i])
        post = post + precv[i].astype(jnp.float32)
    out_ref[...] = layer_norm(post, gain2_ref[...]).astype(jnp.bfloat16)
    for cp in started:
        cp.wait_send()


def local(
    query_one, query_two, key_one, key_two, values, mix_lambda, head_gain, stream, out_weight, first_gain,
    up_weight, down_weight, second_gain,
):
    bf, f32 = jnp.bfloat16, jnp.float32
    hbm = pl.BlockSpec(memory_space=pltpu.HBM)
    dma = pltpu.SemaphoreType.DMA
    return pl.pallas_call(
        layer_kernel,
        out_shape=jax.ShapeDtypeStruct((SUB, 2048), bf),
        in_specs=[pl.BlockSpec(memory_space=pltpu.SMEM)] + [hbm] * 12,
        out_specs=pl.BlockSpec(memory_space=pltpu.VMEM),
        scratch_shapes=[
            pltpu.VMEM((256, 128), bf),
            pltpu.VMEM((256, 128), bf),
            pltpu.VMEM((256, 128), bf),
            pltpu.VMEM((256, 128), bf),
            pltpu.VMEM((256, 256), bf),
            pltpu.VMEM((1, 128), f32),
            pltpu.VMEM((1, 2048), f32),
            pltpu.VMEM((1, 2048), f32),
            pltpu.VMEM((2, 512, 128), bf),
            pltpu.VMEM((2, 128, 256), bf),
            pltpu.VMEM((8, 2, 512, 128), bf),
            pltpu.VMEM((4, 2, 128, 256), bf),
            pltpu.VMEM((16, 128, 256), f32),
            pltpu.VMEM((16, 1, 256), f32),
            pltpu.VMEM((16, 1, 256), f32),
            pltpu.VMEM((16, 256, 256), bf),
            pltpu.VMEM((4, 512, 256), f32),
            pltpu.VMEM((4, 8, 256), f32),
            pltpu.VMEM((3, 4, 128, 256), bf),
            pltpu.VMEM((3, 8, 1, 256), f32),
            pltpu.VMEM((3, 4, 128, 256), bf),
            pltpu.VMEM((3, 8, 1, 256), f32),
            pltpu.VMEM((2, 256, 128), bf),
            pltpu.VMEM((8, SUB, 128), bf),
            pltpu.VMEM((NX, SUB, 512), bf),
            pltpu.VMEM((1024, 2048), bf),
            pltpu.VMEM((NZ, NY, 2, 32, 1024), bf),
            pltpu.VMEM((NZ, NY, 2, 32, 1024), bf),
            pltpu.VMEM((NX, SUB, 2048), bf),
            pltpu.VMEM((3, SUB, 2048), bf),
            pltpu.VMEM((3, SUB, 2048), bf),
            pltpu.VMEM((SUB, 2048), bf),
            dma((96,)),
            dma((12,)),
            dma((8, 2)),
            dma((4, 2)),
            dma((3,)),
            dma((3,)),
            dma((3,)),
            dma((7,)),
            dma((3,)),
            dma((7,)),
            dma((8,)),
            dma((7,)),
            dma((3,)),
            dma((4,)),
            dma((3,)),
            dma((3,)),
            dma((3,)),
            dma((3,)),
            dma((1,)),
        ],
        compiler_params=pltpu.CompilerParams(
            collective_id=0, has_side_effects=True, vmem_limit_bytes=56 * 1024 * 1024
        ),
        cost_estimate=pl.CostEstimate(flops=20_000_000_000, bytes_accessed=4_000_000, transcendentals=17_000_000),
        name="layer",
    )(
        mix_lambda, query_one, query_two, key_one, key_two, values, head_gain.reshape(1, 128), stream, out_weight,
        first_gain.reshape(1, 2048), up_weight, down_weight.T, second_gain.reshape(1, 2048),
    )


def solution(mesh):
    in_specs = (
        P("sp", "tp"), P("sp", "tp"), P("sp", "tp"), P("sp", "tp"), P("sp", "tp"), P("tp"), P(), P("sp", "tp"),
        P("tp", None), P(), P("sp", "tp"), P("tp", "sp"), P(),
    )
    return jax.shard_map(
        local, mesh=mesh, in_specs=in_specs, out_specs=P(("sp", "tp"), None), check_vma=False
    )
```

```python
import functools

import jax
import jax.numpy as jnp
from jax import lax
from jax.experimental import pallas as pl
from jax.experimental.pallas import tpu as pltpu
from jax.sharding import PartitionSpec as P

MESH = pl.DeviceIdType.MESH
NZ, NY, NX = 8, 4, 4
ALPHA = 2.0**0.5
LOG2E = 1.4426950408889634
CEXP = LOG2E * 64 ** (-0.5)
LOW = -1e30
TOK = 256
SUB = 64
NT = (((1,), (1,)), ((), ()))


def layer_norm(value, gain):
    centre = jnp.mean(value, axis=-1, keepdims=True)
    spread = jnp.mean(jnp.square(value - centre), axis=-1, keepdims=True)
    return (value - centre) * lax.rsqrt(spread + 1e-05) * gain


def layer_kernel(
    lam_ref, q1_hbm, q2_hbm, k1_hbm, k2_hbm, v_hbm, hgain_hbm, stream_hbm, ow_hbm, gain1_hbm, up_hbm, down_hbm, gain2_hbm,
    out_ref,
    q1_ref, q2_ref, k1_ref, k2_ref, v_ref, gain_ref, gain1_ref, gain2_ref,
    kvsrc, qsrc, kvbuf, qbuf, acc, mbuf, lbuf, qexp, sbuf, topbuf, osend, ssend, orecv, srecv, attown, attbuf, strbuf,
    wout, wup, wdn, hid, psend, precv, pown, prelay, orelay, srelay, wdnt,
    snd, loc, kv_rcv, q_rcv, o_rcv, s_rcv, str_rcv, att_rcv,
    upy_rcv, upz_rcv, updd_rcv, dnz_rcv, dny_rcv, dndd_rcv, ow_rcv, owdd_rcv, hid_rcv, p_rcv, pr_rcv, or_rcv,
):
    sp = lax.axis_index("sp")
    x = lax.axis_index("tp")
    c = lax.rem(sp, 2)
    y = lax.rem(sp // 2, NY)
    z = sp // (2 * NY)
    f = 1 - 2 * c

    def at_z(d):
        return lax.rem(z + (d + NZ), NZ)

    def at_y(d):
        return lax.rem(y + (d + NY), NY)

    def at_x(d):
        return lax.rem(x + (d + NX), NX)

    def dev(dz=0, dy=0, core=None, dx=0):
        cc = c if core is None else core
        return {"sp": (at_z(dz) * NY + at_y(dy)) * 2 + cc, "tp": at_x(dx)}

    sibling = dev(core=1 - c)
    started = []

    def send(src, dst, rcv, to):
        cp = pltpu.make_async_remote_copy(
            src_ref=src, dst_ref=dst, send_sem=snd.at[len(started)], recv_sem=rcv, device_id=to, device_id_type=MESH
        )
        cp.start()
        started.append(cp)

    def arrived(dst, rcv):
        pltpu.make_async_remote_copy(
            src_ref=dst, dst_ref=dst, send_sem=snd.at[0], recv_sem=rcv, device_id=sibling, device_id_type=MESH
        ).wait_recv()

    mine = pl.ds(pl.multiple_of(x * SUB, SUB), SUB)

    def ow_rows(d, half):
        return pl.ds(pl.multiple_of((2 * at_x(d) + half) * 128, 128), 128)

    local_pairs = [
        (q1_hbm, q1_ref), (q2_hbm, q2_ref), (k1_hbm, k1_ref), (k2_hbm, k2_ref), (v_hbm, v_ref),
        (hgain_hbm, gain_ref), (gain1_hbm, gain1_ref), (gain2_hbm, gain2_ref),
        (stream_hbm.at[mine, :], strbuf.at[x]),
        (up_hbm, wup.at[z, y, c]), (down_hbm, wdn.at[z, y, c]),
        (ow_hbm, wout.at[pl.ds(pl.multiple_of(x * 256, 256), 256), :]),
    ]
    locals_ = [pltpu.make_async_copy(a, b, loc.at[i]) for i, (a, b) in enumerate(local_pairs)]
    for cp in locals_:
        cp.start()

    barrier = pltpu.get_barrier_semaphore()
    partners = [sibling, dev(dy=2)]
    for core in (0, 1):
        partners += [dev(dz=1, core=core), dev(dz=-1, core=core), dev(dy=1, core=core), dev(dy=-1, core=core)]
        partners += [dev(dx=d, core=core) for d in (1, 2, 3)]
    for p in partners:
        pl.semaphore_signal(barrier, inc=1, device_id=p, device_id_type=MESH)

    mbuf[...] = jnp.full(mbuf.shape, LOW, jnp.float32)
    lbuf[...] = jnp.zeros(lbuf.shape, jnp.float32)

    def clear(i, carry):
        acc[i] = jnp.zeros(acc.shape[1:], jnp.float32)
        return carry

    lax.fori_loop(0, acc.shape[0], clear, 0)
    for cp in locals_[:5]:
        cp.wait()

    lane = lax.broadcasted_iota(jnp.int32, (TOK, 128), 1)
    low_half = lane < 64
    q1t = q1_ref[...].astype(jnp.float32).T.astype(jnp.bfloat16)
    q2t = q2_ref[...].astype(jnp.float32).T.astype(jnp.bfloat16)
    for h in (0, 1):
        qsrc[h, 0:64, :] = q1t[64 * h : 64 * h + 64]
        qsrc[h, 64:128, :] = q2t[64 * h : 64 * h + 64]
    vt = v_ref[...].astype(jnp.float32).T.astype(jnp.bfloat16)
    one, two = k1_ref[...].astype(jnp.float32), k2_ref[...].astype(jnp.float32)
    kvsrc[0, 0:256, :] = jnp.where(low_half, one, pltpu.roll(two, 64, 1)).astype(jnp.bfloat16)
    kvsrc[1, 0:256, :] = jnp.where(low_half, pltpu.roll(one, 64, 1), two).astype(jnp.bfloat16)
    for h in (0, 1):
        kvsrc[h, 256:384, :] = vt[128 * h : 128 * h + 128, 0:128]
        kvsrc[h, 384:512, :] = vt[128 * h : 128 * h + 128, 128:256]
    kvbuf[0, c] = kvsrc[c]
    qbuf[0, c] = qsrc[c]
    pl.semaphore_wait(barrier, len(partners))

    send(qsrc.at[1 - c], qbuf.at[0, c], q_rcv.at[0, c], sibling)
    send(kvsrc.at[1 - c], kvbuf.at[0, c], kv_rcv.at[0, c], sibling)
    for i, d in enumerate((1, -1)):
        send(down_hbm, wdn.at[z, y, c], dnz_rcv.at[i], dev(dz=d))
    for h in (0, 1):
        send(qsrc.at[h], qbuf.at[1, c], q_rcv.at[1, c], dev(dy=1, core=h))
        send(qsrc.at[h], qbuf.at[2, c], q_rcv.at[2, c], dev(dy=-1, core=h))
        send(kvsrc.at[h], kvbuf.at[1, c], kv_rcv.at[1, c], dev(dz=1, core=h))
        send(kvsrc.at[h], kvbuf.at[2, c], kv_rcv.at[2, c], dev(dz=-1, core=h))
    for dx in (1, 2, 3):
        rows = pl.ds(pl.multiple_of(at_x(dx) * SUB, SUB), SUB)
        send(stream_hbm.at[rows, :], strbuf.at[x], str_rcv.at[dx - 1], dev(dx=dx))
    half_rows = pl.ds(pl.multiple_of(c * 128, 128), 128)
    for i, d in enumerate((1, -1)):
        send(up_hbm, wup.at[z, y, c], upy_rcv.at[i], dev(dy=d))
        send(ow_hbm.at[half_rows, :], wout.at[ow_rows(0, c), :], ow_rcv.at[i], dev(dx=d))

    def out_weight_on():
        arrived(wout.at[ow_rows(-1, c), :], ow_rcv.at[0])
        arrived(wout.at[ow_rows(1, c), :], ow_rcv.at[1])
        blk = wout.at[ow_rows(-f, c), :]
        send(blk, blk, ow_rcv.at[2], dev(dx=f))
        for i, d in enumerate((-1, 1)):
            blk = wout.at[ow_rows(d, c), :]
            send(blk, blk, owdd_rcv.at[i], sibling)

    def out_weight_end():
        blk = wout.at[ow_rows(2, c), :]
        arrived(blk, ow_rcv.at[2])
        send(blk, blk, owdd_rcv.at[2], sibling)

    def up_y_on():
        arrived(wup.at[z, at_y(-1), c], upy_rcv.at[0])
        arrived(wup.at[z, at_y(1), c], upy_rcv.at[1])
        blk = wup.at[z, at_y(-f), c]
        send(blk, blk, upy_rcv.at[2], dev(dy=f))

    def up_y_end():
        arrived(wup.at[z, at_y(2), c], upy_rcv.at[2])
        locals_[9].wait()

    def up_z_start():
        blk = wup.at[z, :, c]
        for i, d in enumerate((1, -1)):
            send(blk, blk, upz_rcv.at[i], dev(dz=d))
        send(blk, blk, updd_rcv.at[0], sibling)

    def up_z_step(d):
        if d == 4:
            blk = wup.at[at_z(4), :, c]
            arrived(blk, upz_rcv.at[6])
            send(blk, blk, updd_rcv.at[7], sibling)
            return
        for i, s in enumerate((-1, 1)):
            blk = wup.at[at_z(s * d), :, c]
            arrived(blk, upz_rcv.at[2 * (d - 1) + i])
            if d < 3:
                send(blk, blk, upz_rcv.at[2 * d + i], dev(dz=-s))
        if d == 3:
            blk = wup.at[at_z(-3 * f), :, c]
            send(blk, blk, upz_rcv.at[6], dev(dz=f))
        for i, s in enumerate((-1, 1)):
            blk = wup.at[at_z(s * d), :, c]
            send(blk, blk, updd_rcv.at[2 * (d - 1) + 1 + i], sibling)

    def down_z_step(d):
        if d == 4:
            arrived(wdn.at[at_z(4), y, c], dnz_rcv.at[6])
            return
        for i, s in enumerate((-1, 1)):
            blk = wdn.at[at_z(s * d), y, c]
            arrived(blk, dnz_rcv.at[2 * (d - 1) + i])
            if d < 3:
                send(blk, blk, dnz_rcv.at[2 * d + i], dev(dz=-s))
        if d == 3:
            blk = wdn.at[at_z(-3 * f), y, c]
            send(blk, blk, dnz_rcv.at[6], dev(dz=f))

    def down_y_start():
        locals_[10].wait()
        blk = wdn.at[:, y, c]
        for i, d in enumerate((1, -1)):
            send(blk, blk, dny_rcv.at[i], dev(dy=d))
        send(blk, blk, dndd_rcv.at[0], sibling)

    def down_y_on():
        arrived(wdn.at[:, at_y(-1), c], dny_rcv.at[0])
        arrived(wdn.at[:, at_y(1), c], dny_rcv.at[1])
        blk = wdn.at[:, at_y(-f), c]
        send(blk, blk, dny_rcv.at[2], dev(dy=f))
        for i, d in enumerate((-1, 1)):
            blk = wdn.at[:, at_y(d), c]
            send(blk, blk, dndd_rcv.at[1 + i], sibling)

    def down_y_end():
        blk = wdn.at[:, at_y(2), c]
        arrived(blk, dny_rcv.at[2])
        send(blk, blk, dndd_rcv.at[3], sibling)

    def take_kv(slot):
        for cc in (0, 1):
            arrived(kvbuf.at[slot, cc], kv_rcv.at[slot, cc])
            step = 1 if slot % 2 else -1
            if slot <= 4:
                send(kvbuf.at[slot, cc], kvbuf.at[slot + 2, cc], kv_rcv.at[slot + 2, cc], dev(dz=step))
            elif (slot, cc) in ((5, 0), (6, 1)):
                send(kvbuf.at[slot, cc], kvbuf.at[7, cc], kv_rcv.at[7, cc], dev(dz=step))

    def take_q(slot):
        for cc in (0, 1):
            arrived(qbuf.at[slot, cc], q_rcv.at[slot, cc])
            if (slot, cc) in ((1, 0), (2, 1)):
                send(qbuf.at[slot, cc], qbuf.at[3, cc], q_rcv.at[3, cc], dev(dy=1 if slot == 1 else -1))

    def expand(qs):
        for cc in (0, 1):
            scaled = qbuf[qs, cc].astype(jnp.float32) * CEXP
            high = scaled.astype(jnp.bfloat16)
            rest = (scaled - high.astype(jnp.float32)).astype(jnp.bfloat16)
            blank = jnp.zeros((64, 256), jnp.bfloat16)
            for mp in (0, 1):
                own = slice(64 * mp, 64 * mp + 64)
                other = slice(64 - 64 * mp, 128 - 64 * mp)
                at = qs * 4 + 2 * cc + mp
                qexp[at, own, :] = high[own]
                qexp[at, other, :] = blank
                own = slice(128 + 64 * mp, 192 + 64 * mp)
                other = slice(192 - 64 * mp, 256 - 64 * mp)
                qexp[at, own, :] = rest[64 * mp : 64 * mp + 64]
                qexp[at, other, :] = blank

    def score(kvs, qs, j):
        slot = j % 4
        keys = jnp.concatenate([kvbuf[kvs, cc, 0:256, :] for cc in (0, 1)], axis=0)
        keys = jnp.concatenate([keys, keys], axis=1)
        scores = jnp.dot(keys, qexp[qs * 4 + j], preferred_element_type=jnp.float32)
        sbuf[slot] = scores
        topbuf[slot] = jnp.max(scores.reshape(64, 8, 256), axis=0)

    def absorb(kvs, qs, j):
        slot = j % 4
        at = qs * 4 + j
        vals = jnp.concatenate(
            [kvbuf[kvs, cc, 256 + 128 * i : 384 + 128 * i, :] for cc in (0, 1) for i in (0, 1)], axis=1
        )
        old = mbuf[at]
        new = jnp.maximum(old, jnp.max(topbuf[slot], axis=0, keepdims=True))
        factor = jnp.exp2(old - new)
        expo = jnp.exp2(sbuf[slot] - new)
        mbuf[at] = new
        lbuf[at] = lbuf[at] * factor + jnp.sum(expo, axis=0, keepdims=True)
        acc[at] = acc[at] * factor + jnp.dot(vals, expo.astype(jnp.bfloat16), preferred_element_type=jnp.float32)

    def process(kv_lo, kv_n, q_lo, q_n, ready=False, then=None):
        last = kv_n * q_n - 1

        def place(i):
            return kv_lo + i // q_n, q_lo + lax.rem(i, q_n)

        def trip(i, carry):
            kvs, qs = place(i)
            nkvs, nqs = place(jnp.minimum(i + 1, last))
            if then is not None:
                nkvs, nqs = jnp.where(i == last, then[0], nkvs), jnp.where(i == last, then[1], nqs)
            for j in range(4):
                if j < 2:
                    score(kvs, qs, j + 2)
                else:
                    score(nkvs, nqs, j - 2)
                absorb(kvs, qs, j)
            return carry

        if not ready:
            score(kv_lo, q_lo, 0)
            score(kv_lo, q_lo, 1)
        lax.fori_loop(0, last + 1, trip, 0)

    q_direct, q_merged = (3 - f) // 2, (3 + f) // 2

    def finish(qs, place):
        for i in range(4):
            osend[place, i] = (acc[qs * 4 + i] / lbuf[qs * 4 + i]).astype(jnp.bfloat16)
        for i in range(4):
            ssend[place, i] = mbuf[qs * 4 + i]
            ssend[place, 4 + i] = lbuf[qs * 4 + i]

    def opposite_out():
        finish(3, 0)
        send(osend.at[0], orelay, or_rcv.at[0], dev(dy=f))
        send(ssend.at[0], srelay, or_rcv.at[1], dev(dy=f))

    def direct_out():
        finish(q_direct, 1)
        send(osend.at[1], orecv.at[0], o_rcv.at[0], dev(dy=-f))
        send(ssend.at[1], srecv.at[0], s_rcv.at[0], dev(dy=-f))

    def merged_out():
        arrived(orelay, or_rcv.at[0])
        arrived(srelay, or_rcv.at[1])
        for i in range(4):
            m, l = mbuf[q_merged * 4 + i], lbuf[q_merged * 4 + i]
            top = jnp.maximum(m, srelay[i])
            w, v = jnp.exp2(m - top), jnp.exp2(srelay[i] - top) * srelay[4 + i]
            total = l * w + v
            osend[2, i] = (
                acc[q_merged * 4 + i] * (w / total) + orelay[i].astype(jnp.float32) * (v / total)
            ).astype(jnp.bfloat16)
            ssend[2, i] = top
            ssend[2, 4 + i] = total
        send(osend.at[2], orecv.at[1], o_rcv.at[1], dev(dy=f))
        send(ssend.at[2], srecv.at[1], s_rcv.at[1], dev(dy=f))

    arrived(qbuf.at[0, 1 - c], q_rcv.at[0, 1 - c])
    expand(0)
    arrived(kvbuf.at[0, 1 - c], kv_rcv.at[0, 1 - c])
    process(0, 1, 0, 1)
    down_z_step(1)
    take_q(1)
    take_q(2)
    expand(1)
    expand(2)
    process(0, 1, 1, 2)
    down_z_step(2)
    take_kv(1)
    take_kv(2)
    up_y_on()
    process(1, 1, 0, 3)
    take_q(3)
    expand(3)
    down_z_step(3)
    process(0, 2, 3, 1)
    take_kv(3)
    take_kv(4)
    down_z_step(4)
    down_y_start()
    out_weight_on()
    up_y_end()
    process(2, 1, 0, 4, then=(3, 0))
    up_z_start()
    process(3, 1, 0, 4, ready=True)
    take_kv(5)
    take_kv(6)
    process(4, 1, 0, 4, then=(5, 3))
    process(5, 2, 3, 1, ready=True, then=(5, q_direct))
    process(5, 2, q_direct, 1, ready=True)
    out_weight_end()
    take_kv(7)
    process(7, 1, 3, 1, then=(7, q_direct))
    opposite_out()
    process(7, 1, q_direct, 1, ready=True, then=(5, q_merged))
    direct_out()
    up_z_step(1)
    process(5, 3, q_merged, 1, ready=True, then=(5, 0))
    process(5, 3, 0, 1, ready=True)
    merged_out()
    down_y_on()
    up_z_step(2)

    for j in (0, 1):
        arrived(orecv.at[j], o_rcv.at[j])
        arrived(srecv.at[j], s_rcv.at[j])
    locals_[5].wait()
    lam = lam_ref[c]
    gain = gain_ref[...] * 0.8
    for cc in (0, 1):
        maps = []
        for mp in (0, 1):
            i = 2 * cc + mp
            ms = [mbuf[i]] + [srecv[j, i] for j in range(2)]
            ls = [lbuf[i]] + [srecv[j, 4 + i] for j in range(2)]
            top = functools.reduce(jnp.maximum, ms)
            ws = [jnp.exp2(m - top) for m in ms]
            total = ws[0] * ls[0]
            out = acc[i] * ws[0]
            for j in range(2):
                w = ws[j + 1] * ls[j + 1]
                total = total + w
                out = out + orecv[j, i].astype(jnp.float32) * w
            maps.append(out / total)
        mixed = maps[0] - lam * maps[1]
        inv = lax.rsqrt(jnp.mean(mixed * mixed, axis=0, keepdims=True) + 1e-5)
        attown[cc] = ((mixed * inv).T * gain).astype(jnp.bfloat16)


    head = 2 * x + c
    for dx in range(NX):
        for dc in (0, 1):
            if dx == 0 and dc == 0:
                continue
            cc = c if dc == 0 else 1 - c
            rows = pl.ds(pl.multiple_of(at_x(dx) * SUB, SUB), SUB)
            send(attown.at[cc, rows, :], attbuf.at[head], att_rcv.at[2 * dx + dc - 1], dev(dx=dx, core=cc))
    attbuf[head] = attown[c, mine, :]
    up_z_step(3)
    for i in range(3):
        arrived(wout.at[ow_rows((-1, 1, 2)[i], 1 - c), :], owdd_rcv.at[i])
    for i in (6, 7, 8, 11):
        locals_[i].wait()
    for dx in (1, 2, 3):
        arrived(strbuf.at[at_x(-dx)], str_rcv.at[dx - 1])
    for dx in range(NX):
        for dc in (0, 1):
            if dx == 0 and dc == 0:
                continue
            cc = c if dc == 0 else 1 - c
            arrived(attbuf.at[2 * at_x(-dx) + cc], att_rcv.at[2 * dx + dc - 1])
    attended = jnp.concatenate([attbuf[h] for h in range(8)], axis=1)
    rows = jnp.concatenate([strbuf[i] for i in range(NX)], axis=1).astype(jnp.float32)
    pre = ALPHA * rows + jnp.dot(attended, wout[...], preferred_element_type=jnp.float32)
    own = layer_norm(pre, gain1_ref[...]).astype(jnp.bfloat16)
    hid[x] = own
    down_y_end()
    halves = [pl.ds(i * (SUB // 2), SUB // 2) for i in (0, 1)]
    for n, half in enumerate(halves):
        for i, d in enumerate((f, -f)):
            send(hid.at[x, half, :], hid.at[x, half, :], hid_rcv.at[2 * i + n], dev(dx=d))
    up_z_step(4)
    arrived(wdn.at[:, y, 1 - c], dndd_rcv.at[0])
    for i, d in enumerate((-1, 1)):
        arrived(wdn.at[:, at_y(d), 1 - c], dndd_rcv.at[1 + i])
    arrived(wdn.at[:, at_y(2), 1 - c], dndd_rcv.at[3])
    for i in range(NZ):
        wdnt[:, 256 * i : 256 * i + 256] = wdn[i].reshape(256, 1024).T
    arrived(wup.at[z, :, 1 - c], updd_rcv.at[0])
    for d in (1, 2, 3):
        for i, s in enumerate((-1, 1)):
            arrived(wup.at[at_z(s * d), :, 1 - c], updd_rcv.at[2 * (d - 1) + 1 + i])
    arrived(wup.at[at_z(4), :, 1 - c], updd_rcv.at[7])

    def mixer(tokens):
        total = None
        for n in range(4):
            up = wup[:, :, :, :, 256 * n : 256 * n + 256].reshape(2048, 256)
            upper = jnp.dot(tokens, up, preferred_element_type=jnp.float32)
            act = jnp.square(jnp.maximum(upper, 0.0)).astype(jnp.bfloat16)
            part = jnp.dot(act, wdnt[256 * n : 256 * n + 256, :], preferred_element_type=jnp.float32)
            total = part if total is None else total + part
        return total

    post = mixer(own) + ALPHA * own.astype(jnp.float32)
    for n, half in enumerate(halves):
        blk = hid.at[at_x(-f), half, :]
        arrived(blk, hid_rcv.at[n])
        send(blk, blk, hid_rcv.at[4 + n], dev(dx=f))
    for n, half in enumerate(halves):
        arrived(hid.at[at_x(f), half, :], hid_rcv.at[2 + n])
    both = mixer(jnp.concatenate([hid[at_x(-f)], hid[at_x(f)]], axis=0))
    psend[0] = both[0:SUB].astype(jnp.bfloat16)
    pown[...] = both[SUB:]
    send(psend.at[0], precv.at[0], p_rcv.at[0], dev(dx=-f))
    for n, half in enumerate(halves):
        arrived(hid.at[at_x(2), half, :], hid_rcv.at[4 + n])
    psend[1] = mixer(hid[at_x(2)]).astype(jnp.bfloat16)
    quarters = [pl.ds(i * (SUB // 4), SUB // 4) for i in range(4)]
    for i, part in enumerate(quarters):
        send(psend.at[1, part, :], prelay.at[i], pr_rcv.at[i], dev(dx=f))
    for i, part in enumerate(quarters):
        arrived(prelay.at[i], pr_rcv.at[i])
        psend[2, part, :] = (pown[part, :] + prelay[i].astype(jnp.float32)).astype(jnp.bfloat16)
        send(psend.at[2, part, :], precv.at[1, part, :], p_rcv.at[1 + i], dev(dx=f))
    arrived(precv.at[0], p_rcv.at[0])
    for i, part in enumerate(quarters):
        arrived(precv.at[1, part, :], p_rcv.at[1 + i])
    for i in range(2):
        post = post + precv[i].astype(jnp.float32)
    out_ref[...] = layer_norm(post, gain2_ref[...]).astype(jnp.bfloat16)
    for cp in started:
        cp.wait_send()


def local(
    query_one, query_two, key_one, key_two, values, mix_lambda, head_gain, stream, out_weight, first_gain,
    up_weight, down_weight, second_gain,
):
    bf, f32 = jnp.bfloat16, jnp.float32
    hbm = pl.BlockSpec(memory_space=pltpu.HBM)
    dma = pltpu.SemaphoreType.DMA
    return pl.pallas_call(
        layer_kernel,
        out_shape=jax.ShapeDtypeStruct((SUB, 2048), bf),
        in_specs=[pl.BlockSpec(memory_space=pltpu.SMEM)] + [hbm] * 12,
        out_specs=pl.BlockSpec(memory_space=pltpu.VMEM),
        scratch_shapes=[
            pltpu.VMEM((256, 128), bf),
            pltpu.VMEM((256, 128), bf),
            pltpu.VMEM((256, 128), bf),
            pltpu.VMEM((256, 128), bf),
            pltpu.VMEM((256, 256), bf),
            pltpu.VMEM((1, 128), f32),
            pltpu.VMEM((1, 2048), f32),
            pltpu.VMEM((1, 2048), f32),
            pltpu.VMEM((2, 512, 128), bf),
            pltpu.VMEM((2, 128, 256), bf),
            pltpu.VMEM((8, 2, 512, 128), bf),
            pltpu.VMEM((4, 2, 128, 256), bf),
            pltpu.VMEM((16, 128, 256), f32),
            pltpu.VMEM((16, 1, 256), f32),
            pltpu.VMEM((16, 1, 256), f32),
            pltpu.VMEM((16, 256, 256), bf),
            pltpu.VMEM((4, 512, 256), f32),
            pltpu.VMEM((4, 8, 256), f32),
            pltpu.VMEM((3, 4, 128, 256), bf),
            pltpu.VMEM((3, 8, 1, 256), f32),
            pltpu.VMEM((2, 4, 128, 256), bf),
            pltpu.VMEM((2, 8, 1, 256), f32),
            pltpu.VMEM((2, 256, 128), bf),
            pltpu.VMEM((8, SUB, 128), bf),
            pltpu.VMEM((NX, SUB, 512), bf),
            pltpu.VMEM((1024, 2048), bf),
            pltpu.VMEM((NZ, NY, 2, 32, 1024), bf),
            pltpu.VMEM((NZ, NY, 2, 32, 1024), bf),
            pltpu.VMEM((NX, SUB, 2048), bf),
            pltpu.VMEM((3, SUB, 2048), bf),
            pltpu.VMEM((2, SUB, 2048), bf),
            pltpu.VMEM((SUB, 2048), f32),
            pltpu.VMEM((4, SUB // 4, 2048), bf),
            pltpu.VMEM((4, 128, 256), bf),
            pltpu.VMEM((8, 1, 256), f32),
            pltpu.VMEM((1024, 2048), bf),
            dma((128,)),
            dma((12,)),
            dma((8, 2)),
            dma((4, 2)),
            dma((3,)),
            dma((3,)),
            dma((3,)),
            dma((7,)),
            dma((3,)),
            dma((7,)),
            dma((8,)),
            dma((7,)),
            dma((3,)),
            dma((4,)),
            dma((3,)),
            dma((3,)),
            dma((6,)),
            dma((6,)),
            dma((4,)),
            dma((2,)),
        ],
        compiler_params=pltpu.CompilerParams(
            collective_id=0, has_side_effects=True, vmem_limit_bytes=56 * 1024 * 1024
        ),
        cost_estimate=pl.CostEstimate(flops=20_000_000_000, bytes_accessed=4_000_000, transcendentals=17_000_000),
        name="layer",
    )(
        mix_lambda, query_one, query_two, key_one, key_two, values, head_gain.reshape(1, 128), stream, out_weight,
        first_gain.reshape(1, 2048), up_weight, down_weight.T, second_gain.reshape(1, 2048),
    )


def solution(mesh):
    in_specs = (
        P("sp", "tp"), P("sp", "tp"), P("sp", "tp"), P("sp", "tp"), P("sp", "tp"), P("tp"), P(), P("sp", "tp"),
        P("tp", None), P(), P("sp", "tp"), P("tp", "sp"), P(),
    )
    return jax.shard_map(
        local, mesh=mesh, in_specs=in_specs, out_specs=P(("sp", "tp"), None), check_vma=False
    )
```

```python
import functools

import jax
import jax.numpy as jnp
from jax import lax
from jax.experimental import pallas as pl
from jax.experimental.pallas import tpu as pltpu
from jax.sharding import PartitionSpec as P

MESH = pl.DeviceIdType.MESH
NZ, NY, NX = 8, 4, 4
ALPHA = 2.0**0.5
LOG2E = 1.4426950408889634
CEXP = LOG2E * 64 ** (-0.5)
LOW = -1e30
TOK = 256
SUB = 64
NT = (((1,), (1,)), ((), ()))


def layer_norm(value, gain):
    centre = jnp.mean(value, axis=-1, keepdims=True)
    spread = jnp.mean(jnp.square(value - centre), axis=-1, keepdims=True)
    return (value - centre) * lax.rsqrt(spread + 1e-05) * gain


def layer_kernel(
    lam_ref, q1_hbm, q2_hbm, k1_hbm, k2_hbm, v_hbm, hgain_hbm, stream_hbm, ow_hbm, gain1_hbm, up_hbm, down_hbm, gain2_hbm,
    out_ref,
    q1_ref, q2_ref, k1_ref, k2_ref, v_ref, gain_ref, gain1_ref, gain2_ref,
    kvsrc, qsrc, kvbuf, qbuf, acc, mbuf, lbuf, qexp, sbuf, topbuf, osend, ssend, orecv, srecv, attown, attbuf, strbuf,
    wout, wup, wdn, hid, psend, precv, pown, prelay, orelay, srelay, wdnt,
    snd, loc, kv_rcv, q_rcv, o_rcv, s_rcv, str_rcv, att_rcv,
    upy_rcv, upz_rcv, updd_rcv, dnz_rcv, dny_rcv, dndd_rcv, ow_rcv, owdd_rcv, hid_rcv, p_rcv, pr_rcv, or_rcv,
):
    sp = lax.axis_index("sp")
    x = lax.axis_index("tp")
    c = lax.rem(sp, 2)
    y = lax.rem(sp // 2, NY)
    z = sp // (2 * NY)
    f = 1 - 2 * c

    def at_z(d):
        return lax.rem(z + (d + NZ), NZ)

    def at_y(d):
        return lax.rem(y + (d + NY), NY)

    def at_x(d):
        return lax.rem(x + (d + NX), NX)

    def dev(dz=0, dy=0, core=None, dx=0):
        cc = c if core is None else core
        return {"sp": (at_z(dz) * NY + at_y(dy)) * 2 + cc, "tp": at_x(dx)}

    sibling = dev(core=1 - c)
    started = []

    def send(src, dst, rcv, to):
        cp = pltpu.make_async_remote_copy(
            src_ref=src, dst_ref=dst, send_sem=snd.at[len(started)], recv_sem=rcv, device_id=to, device_id_type=MESH
        )
        cp.start()
        started.append(cp)

    def arrived(dst, rcv):
        pltpu.make_async_remote_copy(
            src_ref=dst, dst_ref=dst, send_sem=snd.at[0], recv_sem=rcv, device_id=sibling, device_id_type=MESH
        ).wait_recv()

    mine = pl.ds(pl.multiple_of(x * SUB, SUB), SUB)

    def ow_rows(d, half):
        return pl.ds(pl.multiple_of((2 * at_x(d) + half) * 128, 128), 128)

    local_pairs = [
        (q1_hbm, q1_ref), (q2_hbm, q2_ref), (k1_hbm, k1_ref), (k2_hbm, k2_ref), (v_hbm, v_ref),
        (hgain_hbm, gain_ref), (gain1_hbm, gain1_ref), (gain2_hbm, gain2_ref),
        (stream_hbm.at[mine, :], strbuf.at[x]),
        (up_hbm, wup.at[z, y, c]), (down_hbm, wdn.at[z, y, c]),
        (ow_hbm, wout.at[pl.ds(pl.multiple_of(x * 256, 256), 256), :]),
    ]
    locals_ = [pltpu.make_async_copy(a, b, loc.at[i]) for i, (a, b) in enumerate(local_pairs)]
    for cp in locals_:
        cp.start()

    barrier = pltpu.get_barrier_semaphore()
    partners = [sibling, dev(dy=2)]
    for core in (0, 1):
        partners += [dev(dz=1, core=core), dev(dz=-1, core=core), dev(dy=1, core=core), dev(dy=-1, core=core)]
        partners += [dev(dx=d, core=core) for d in (1, 2, 3)]
    for p in partners:
        pl.semaphore_signal(barrier, inc=1, device_id=p, device_id_type=MESH)

    mbuf[...] = jnp.full(mbuf.shape, LOW, jnp.float32)
    lbuf[...] = jnp.zeros(lbuf.shape, jnp.float32)

    def clear(i, carry):
        acc[i] = jnp.zeros(acc.shape[1:], jnp.float32)
        return carry

    lax.fori_loop(0, acc.shape[0], clear, 0)
    for cp in locals_[:5]:
        cp.wait()

    lane = lax.broadcasted_iota(jnp.int32, (TOK, 128), 1)
    low_half = lane < 64
    q1t = q1_ref[...].astype(jnp.float32).T.astype(jnp.bfloat16)
    q2t = q2_ref[...].astype(jnp.float32).T.astype(jnp.bfloat16)
    for h in (0, 1):
        qsrc[h, 0:64, :] = q1t[64 * h : 64 * h + 64]
        qsrc[h, 64:128, :] = q2t[64 * h : 64 * h + 64]
    vt = v_ref[...].astype(jnp.float32).T.astype(jnp.bfloat16)
    one, two = k1_ref[...].astype(jnp.float32), k2_ref[...].astype(jnp.float32)
    kvsrc[0, 0:256, :] = jnp.where(low_half, one, pltpu.roll(two, 64, 1)).astype(jnp.bfloat16)
    kvsrc[1, 0:256, :] = jnp.where(low_half, pltpu.roll(one, 64, 1), two).astype(jnp.bfloat16)
    for h in (0, 1):
        kvsrc[h, 256:384, :] = vt[128 * h : 128 * h + 128, 0:128]
        kvsrc[h, 384:512, :] = vt[128 * h : 128 * h + 128, 128:256]
    kvbuf[0, c] = kvsrc[c]
    qbuf[0, c] = qsrc[c]
    for i in (9, 10, 11):
        locals_[i].wait()
    pl.semaphore_wait(barrier, len(partners))

    send(qsrc.at[1 - c], qbuf.at[0, c], q_rcv.at[0, c], sibling)
    send(kvsrc.at[1 - c], kvbuf.at[0, c], kv_rcv.at[0, c], sibling)
    for i, d in enumerate((1, -1)):
        send(wdn.at[z, y, c], wdn.at[z, y, c], dnz_rcv.at[i], dev(dz=d))
    for h in (0, 1):
        send(qsrc.at[h], qbuf.at[1, c], q_rcv.at[1, c], dev(dy=1, core=h))
        send(qsrc.at[h], qbuf.at[2, c], q_rcv.at[2, c], dev(dy=-1, core=h))
        send(kvsrc.at[h], kvbuf.at[1, c], kv_rcv.at[1, c], dev(dz=1, core=h))
        send(kvsrc.at[h], kvbuf.at[2, c], kv_rcv.at[2, c], dev(dz=-1, core=h))
    for dx in (1, 2, 3):
        rows = pl.ds(pl.multiple_of(at_x(dx) * SUB, SUB), SUB)
        send(stream_hbm.at[rows, :], strbuf.at[x], str_rcv.at[dx - 1], dev(dx=dx))
    for i, d in enumerate((1, -1)):
        send(wout.at[ow_rows(0, c), :], wout.at[ow_rows(0, c), :], ow_rcv.at[i], dev(dx=d))

    def out_weight_on():
        arrived(wout.at[ow_rows(-1, c), :], ow_rcv.at[0])
        arrived(wout.at[ow_rows(1, c), :], ow_rcv.at[1])
        blk = wout.at[ow_rows(-f, c), :]
        send(blk, blk, ow_rcv.at[2], dev(dx=f))
        for i, d in enumerate((-1, 1)):
            blk = wout.at[ow_rows(d, c), :]
            send(blk, blk, owdd_rcv.at[i], sibling)

    def out_weight_end():
        blk = wout.at[ow_rows(2, c), :]
        arrived(blk, ow_rcv.at[2])
        send(blk, blk, owdd_rcv.at[2], sibling)

    def up_y_start():
        for i, d in enumerate((1, -1)):
            send(wup.at[z, y, c], wup.at[z, y, c], upy_rcv.at[i], dev(dy=d))

    def up_y_on():
        arrived(wup.at[z, at_y(-1), c], upy_rcv.at[0])
        arrived(wup.at[z, at_y(1), c], upy_rcv.at[1])
        blk = wup.at[z, at_y(-f), c]
        send(blk, blk, upy_rcv.at[2], dev(dy=f))

    def up_y_end():
        arrived(wup.at[z, at_y(2), c], upy_rcv.at[2])

    def up_z_start():
        blk = wup.at[z, :, c]
        for i, d in enumerate((1, -1)):
            send(blk, blk, upz_rcv.at[i], dev(dz=d))
        send(blk, blk, updd_rcv.at[0], sibling)

    def up_z_step(d):
        if d == 4:
            blk = wup.at[at_z(4), :, c]
            arrived(blk, upz_rcv.at[6])
            send(blk, blk, updd_rcv.at[7], sibling)
            return
        for i, s in enumerate((-1, 1)):
            blk = wup.at[at_z(s * d), :, c]
            arrived(blk, upz_rcv.at[2 * (d - 1) + i])
            if d < 3:
                send(blk, blk, upz_rcv.at[2 * d + i], dev(dz=-s))
        if d == 3:
            blk = wup.at[at_z(-3 * f), :, c]
            send(blk, blk, upz_rcv.at[6], dev(dz=f))
        for i, s in enumerate((-1, 1)):
            blk = wup.at[at_z(s * d), :, c]
            send(blk, blk, updd_rcv.at[2 * (d - 1) + 1 + i], sibling)

    def down_z_step(d):
        if d == 4:
            arrived(wdn.at[at_z(4), y, c], dnz_rcv.at[6])
            return
        for i, s in enumerate((-1, 1)):
            blk = wdn.at[at_z(s * d), y, c]
            arrived(blk, dnz_rcv.at[2 * (d - 1) + i])
            if d < 3:
                send(blk, blk, dnz_rcv.at[2 * d + i], dev(dz=-s))
        if d == 3:
            blk = wdn.at[at_z(-3 * f), y, c]
            send(blk, blk, dnz_rcv.at[6], dev(dz=f))

    def down_zs(g):
        return {0: ((0, 0),), 1: ((-1, 3), (1, 6)), 2: ((-2, 9), (2, 12)), 3: ((-3, 15), (3, 18)), 4: ((4, 21),)}[g]

    def down_y_start(g):
        for dz, k in down_zs(g):
            blk = wdn.at[at_z(dz), y, c]
            for i, d in enumerate((1, -1)):
                send(blk, blk, dny_rcv.at[k + i], dev(dy=d))

    def down_y_on(g):
        for dz, k in down_zs(g):
            for i, d in enumerate((-1, 1)):
                arrived(wdn.at[at_z(dz), at_y(d), c], dny_rcv.at[k + i])
            blk = wdn.at[at_z(dz), at_y(-f), c]
            send(blk, blk, dny_rcv.at[k + 2], dev(dy=f))

    def down_y_end(g):
        for dz, k in down_zs(g):
            arrived(wdn.at[at_z(dz), at_y(2), c], dny_rcv.at[k + 2])

    def down_over(i):
        blk = wdn.at[:, at_y((0, -1, 1, 2)[i]), c]
        send(blk, blk, dndd_rcv.at[i], sibling)

    def down_here():
        for i, d in enumerate((0, -1, 1, 2)):
            arrived(wdn.at[:, at_y(d), 1 - c], dndd_rcv.at[i])

    def take_kv(slot):
        for cc in (0, 1):
            arrived(kvbuf.at[slot, cc], kv_rcv.at[slot, cc])
            step = 1 if slot % 2 else -1
            if slot <= 4:
                send(kvbuf.at[slot, cc], kvbuf.at[slot + 2, cc], kv_rcv.at[slot + 2, cc], dev(dz=step))
            elif (slot, cc) in ((5, 0), (6, 1)):
                send(kvbuf.at[slot, cc], kvbuf.at[7, cc], kv_rcv.at[7, cc], dev(dz=step))

    def take_q(slot):
        for cc in (0, 1):
            arrived(qbuf.at[slot, cc], q_rcv.at[slot, cc])
            if (slot, cc) in ((1, 0), (2, 1)):
                send(qbuf.at[slot, cc], qbuf.at[3, cc], q_rcv.at[3, cc], dev(dy=1 if slot == 1 else -1))

    def expand(qs):
        for cc in (0, 1):
            scaled = qbuf[qs, cc].astype(jnp.float32) * CEXP
            high = scaled.astype(jnp.bfloat16)
            rest = (scaled - high.astype(jnp.float32)).astype(jnp.bfloat16)
            blank = jnp.zeros((64, 256), jnp.bfloat16)
            for mp in (0, 1):
                own = slice(64 * mp, 64 * mp + 64)
                other = slice(64 - 64 * mp, 128 - 64 * mp)
                at = qs * 4 + 2 * cc + mp
                qexp[at, own, :] = high[own]
                qexp[at, other, :] = blank
                own = slice(128 + 64 * mp, 192 + 64 * mp)
                other = slice(192 - 64 * mp, 256 - 64 * mp)
                qexp[at, own, :] = rest[64 * mp : 64 * mp + 64]
                qexp[at, other, :] = blank

    def score(kvs, qs, j):
        slot = j % 4
        keys = jnp.concatenate([kvbuf[kvs, cc, 0:256, :] for cc in (0, 1)], axis=0)
        keys = jnp.concatenate([keys, keys], axis=1)
        scores = jnp.dot(keys, qexp[qs * 4 + j], preferred_element_type=jnp.float32)
        sbuf[slot] = scores
        topbuf[slot] = jnp.max(scores.reshape(64, 8, 256), axis=0)

    def absorb(kvs, qs, j):
        slot = j % 4
        at = qs * 4 + j
        vals = jnp.concatenate(
            [kvbuf[kvs, cc, 256 + 128 * i : 384 + 128 * i, :] for cc in (0, 1) for i in (0, 1)], axis=1
        )
        old = mbuf[at]
        new = jnp.maximum(old, jnp.max(topbuf[slot], axis=0, keepdims=True))
        factor = jnp.exp2(old - new)
        expo = jnp.exp2(sbuf[slot] - new)
        mbuf[at] = new
        lbuf[at] = lbuf[at] * factor + jnp.sum(expo, axis=0, keepdims=True)
        acc[at] = acc[at] * factor + jnp.dot(vals, expo.astype(jnp.bfloat16), preferred_element_type=jnp.float32)

    def process(kv_lo, kv_n, q_lo, q_n, ready=False, then=None):
        last = kv_n * q_n - 1

        def place(i):
            return kv_lo + i // q_n, q_lo + lax.rem(i, q_n)

        def trip(i, carry):
            kvs, qs = place(i)
            nkvs, nqs = place(jnp.minimum(i + 1, last))
            if then is not None:
                nkvs, nqs = jnp.where(i == last, then[0], nkvs), jnp.where(i == last, then[1], nqs)
            for j in range(4):
                if j < 2:
                    score(kvs, qs, j + 2)
                else:
                    score(nkvs, nqs, j - 2)
                absorb(kvs, qs, j)
            return carry

        if not ready:
            score(kv_lo, q_lo, 0)
            score(kv_lo, q_lo, 1)
        lax.fori_loop(0, last + 1, trip, 0)

    q_direct, q_merged = (3 - f) // 2, (3 + f) // 2

    def finish(qs, place):
        for i in range(4):
            osend[place, i] = (acc[qs * 4 + i] / lbuf[qs * 4 + i]).astype(jnp.bfloat16)
        for i in range(4):
            ssend[place, i] = mbuf[qs * 4 + i]
            ssend[place, 4 + i] = lbuf[qs * 4 + i]

    def opposite_out():
        finish(3, 0)
        send(osend.at[0], orelay, or_rcv.at[0], dev(dy=f))
        send(ssend.at[0], srelay, or_rcv.at[1], dev(dy=f))

    def direct_out():
        finish(q_direct, 1)
        send(osend.at[1], orecv.at[0], o_rcv.at[0], dev(dy=-f))
        send(ssend.at[1], srecv.at[0], s_rcv.at[0], dev(dy=-f))

    def merged_out():
        arrived(orelay, or_rcv.at[0])
        arrived(srelay, or_rcv.at[1])
        for i in range(4):
            m, l = mbuf[q_merged * 4 + i], lbuf[q_merged * 4 + i]
            top = jnp.maximum(m, srelay[i])
            w, v = jnp.exp2(m - top), jnp.exp2(srelay[i] - top) * srelay[4 + i]
            total = l * w + v
            osend[2, i] = (
                acc[q_merged * 4 + i] * (w / total) + orelay[i].astype(jnp.float32) * (v / total)
            ).astype(jnp.bfloat16)
            ssend[2, i] = top
            ssend[2, 4 + i] = total
        send(osend.at[2], orecv.at[1], o_rcv.at[1], dev(dy=f))
        send(ssend.at[2], srecv.at[1], s_rcv.at[1], dev(dy=f))

    arrived(qbuf.at[0, 1 - c], q_rcv.at[0, 1 - c])
    expand(0)
    arrived(kvbuf.at[0, 1 - c], kv_rcv.at[0, 1 - c])
    process(0, 1, 0, 1)
    down_z_step(1)
    take_q(1)
    take_q(2)
    up_y_start()
    down_y_start(0)
    down_y_start(1)
    expand(1)
    expand(2)
    process(0, 1, 1, 2)
    take_kv(1)
    take_kv(2)
    process(1, 1, 0, 3)
    take_q(3)
    expand(3)
    down_z_step(2)
    down_y_start(2)
    process(0, 2, 3, 1)
    take_kv(3)
    take_kv(4)
    up_y_on()
    down_y_on(0)
    process(2, 1, 0, 4, then=(3, 0))
    down_z_step(3)
    down_y_start(3)
    down_y_on(1)
    up_y_end()
    process(3, 1, 0, 4, ready=True)
    take_kv(5)
    take_kv(6)
    up_z_start()
    down_y_on(2)
    out_weight_on()
    process(4, 1, 0, 4, then=(5, 3))
    process(5, 2, 3, 1, ready=True, then=(5, q_direct))
    down_z_step(4)
    down_y_start(4)
    down_y_on(3)
    down_over(0)
    process(5, 2, q_direct, 1, ready=True)
    take_kv(7)
    process(7, 1, 3, 1, then=(7, q_direct))
    opposite_out()
    process(7, 1, q_direct, 1, ready=True, then=(5, q_merged))
    process(5, 3, q_merged, 1, ready=True, then=(5, 0))
    direct_out()
    out_weight_end()
    process(5, 3, 0, 1, ready=True)
    up_z_step(1)
    merged_out()
    down_y_on(4)

    for j in (0, 1):
        arrived(orecv.at[j], o_rcv.at[j])
        arrived(srecv.at[j], s_rcv.at[j])
    locals_[5].wait()
    lam = lam_ref[c]
    gain = gain_ref[...] * 0.8
    for cc in (0, 1):
        maps = []
        for mp in (0, 1):
            i = 2 * cc + mp
            ms = [mbuf[i]] + [srecv[j, i] for j in range(2)]
            ls = [lbuf[i]] + [srecv[j, 4 + i] for j in range(2)]
            top = functools.reduce(jnp.maximum, ms)
            ws = [jnp.exp2(m - top) for m in ms]
            total = ws[0] * ls[0]
            out = acc[i] * ws[0]
            for j in range(2):
                w = ws[j + 1] * ls[j + 1]
                total = total + w
                out = out + orecv[j, i].astype(jnp.float32) * w
            maps.append(out / total)
        mixed = maps[0] - lam * maps[1]
        inv = lax.rsqrt(jnp.mean(mixed * mixed, axis=0, keepdims=True) + 1e-5)
        attown[cc] = ((mixed * inv).T * gain).astype(jnp.bfloat16)


    head = 2 * x + c
    for dx in range(NX):
        for dc in (0, 1):
            if dx == 0 and dc == 0:
                continue
            cc = c if dc == 0 else 1 - c
            rows = pl.ds(pl.multiple_of(at_x(dx) * SUB, SUB), SUB)
            send(attown.at[cc, rows, :], attbuf.at[head], att_rcv.at[2 * dx + dc - 1], dev(dx=dx, core=cc))
    attbuf[head] = attown[c, mine, :]
    up_z_step(2)
    down_over(1)
    down_over(2)
    for i in range(3):
        arrived(wout.at[ow_rows((-1, 1, 2)[i], 1 - c), :], owdd_rcv.at[i])
    for i in (6, 7, 8):
        locals_[i].wait()
    for dx in (1, 2, 3):
        arrived(strbuf.at[at_x(-dx)], str_rcv.at[dx - 1])
    for dx in range(NX):
        for dc in (0, 1):
            if dx == 0 and dc == 0:
                continue
            cc = c if dc == 0 else 1 - c
            arrived(attbuf.at[2 * at_x(-dx) + cc], att_rcv.at[2 * dx + dc - 1])
    attended = jnp.concatenate([attbuf[h] for h in range(8)], axis=1)
    rows = jnp.concatenate([strbuf[i] for i in range(NX)], axis=1).astype(jnp.float32)
    pre = ALPHA * rows + jnp.dot(attended, wout[...], preferred_element_type=jnp.float32)
    own = layer_norm(pre, gain1_ref[...]).astype(jnp.bfloat16)
    hid[x] = own
    halves = [pl.ds(i * (SUB // 2), SUB // 2) for i in (0, 1)]
    for n, half in enumerate(halves):
        send(hid.at[x, half, :], hid.at[x, half, :], hid_rcv.at[n], dev(dx=f))
    for g in range(5):
        down_y_end(g)
    down_over(3)
    up_z_step(3)
    for n, half in enumerate(halves):
        send(hid.at[x, half, :], hid.at[x, half, :], hid_rcv.at[2 + n], dev(dx=-f))
    down_here()
    for i in range(NZ):
        wdnt[:, 256 * i : 256 * i + 256] = wdn[i].reshape(256, 1024).T
    for n, half in enumerate(halves):
        blk = hid.at[at_x(-f), half, :]
        arrived(blk, hid_rcv.at[n])
        send(blk, blk, hid_rcv.at[4 + n], dev(dx=f))
    up_z_step(4)
    arrived(wup.at[z, :, 1 - c], updd_rcv.at[0])
    for d in (1, 2, 3):
        for i, s in enumerate((-1, 1)):
            arrived(wup.at[at_z(s * d), :, 1 - c], updd_rcv.at[2 * (d - 1) + 1 + i])
    arrived(wup.at[at_z(4), :, 1 - c], updd_rcv.at[7])

    def mixer(tokens):
        total = None
        for n in range(4):
            up = wup[:, :, :, :, 256 * n : 256 * n + 256].reshape(2048, 256)
            upper = jnp.dot(tokens, up, preferred_element_type=jnp.float32)
            act = jnp.square(jnp.maximum(upper, 0.0)).astype(jnp.bfloat16)
            part = jnp.dot(act, wdnt[256 * n : 256 * n + 256, :], preferred_element_type=jnp.float32)
            total = part if total is None else total + part
        return total

    post = mixer(own) + ALPHA * own.astype(jnp.float32)
    for n, half in enumerate(halves):
        arrived(hid.at[at_x(f), half, :], hid_rcv.at[2 + n])
    both = mixer(jnp.concatenate([hid[at_x(-f)], hid[at_x(f)]], axis=0))
    psend[0] = both[0:SUB].astype(jnp.bfloat16)
    pown[...] = both[SUB:]
    send(psend.at[0], precv.at[0], p_rcv.at[0], dev(dx=-f))
    for n, half in enumerate(halves):
        arrived(hid.at[at_x(2), half, :], hid_rcv.at[4 + n])
    psend[1] = mixer(hid[at_x(2)]).astype(jnp.bfloat16)
    quarters = [pl.ds(i * (SUB // 4), SUB // 4) for i in range(4)]
    for i, part in enumerate(quarters):
        send(psend.at[1, part, :], prelay.at[i], pr_rcv.at[i], dev(dx=f))
    for i, part in enumerate(quarters):
        arrived(prelay.at[i], pr_rcv.at[i])
        psend[2, part, :] = (pown[part, :] + prelay[i].astype(jnp.float32)).astype(jnp.bfloat16)
        send(psend.at[2, part, :], precv.at[1, part, :], p_rcv.at[1 + i], dev(dx=f))
    arrived(precv.at[0], p_rcv.at[0])
    for i, part in enumerate(quarters):
        arrived(precv.at[1, part, :], p_rcv.at[1 + i])
    for i in range(2):
        post = post + precv[i].astype(jnp.float32)
    out_ref[...] = layer_norm(post, gain2_ref[...]).astype(jnp.bfloat16)
    for cp in started:
        cp.wait_send()


def local(
    query_one, query_two, key_one, key_two, values, mix_lambda, head_gain, stream, out_weight, first_gain,
    up_weight, down_weight, second_gain,
):
    bf, f32 = jnp.bfloat16, jnp.float32
    hbm = pl.BlockSpec(memory_space=pltpu.HBM)
    dma = pltpu.SemaphoreType.DMA
    return pl.pallas_call(
        layer_kernel,
        out_shape=jax.ShapeDtypeStruct((SUB, 2048), bf),
        in_specs=[pl.BlockSpec(memory_space=pltpu.SMEM)] + [hbm] * 12,
        out_specs=pl.BlockSpec(memory_space=pltpu.VMEM),
        scratch_shapes=[
            pltpu.VMEM((256, 128), bf),
            pltpu.VMEM((256, 128), bf),
            pltpu.VMEM((256, 128), bf),
            pltpu.VMEM((256, 128), bf),
            pltpu.VMEM((256, 256), bf),
            pltpu.VMEM((1, 128), f32),
            pltpu.VMEM((1, 2048), f32),
            pltpu.VMEM((1, 2048), f32),
            pltpu.VMEM((2, 512, 128), bf),
            pltpu.VMEM((2, 128, 256), bf),
            pltpu.VMEM((8, 2, 512, 128), bf),
            pltpu.VMEM((4, 2, 128, 256), bf),
            pltpu.VMEM((16, 128, 256), f32),
            pltpu.VMEM((16, 1, 256), f32),
            pltpu.VMEM((16, 1, 256), f32),
            pltpu.VMEM((16, 256, 256), bf),
            pltpu.VMEM((4, 512, 256), f32),
            pltpu.VMEM((4, 8, 256), f32),
            pltpu.VMEM((3, 4, 128, 256), bf),
            pltpu.VMEM((3, 8, 1, 256), f32),
            pltpu.VMEM((2, 4, 128, 256), bf),
            pltpu.VMEM((2, 8, 1, 256), f32),
            pltpu.VMEM((2, 256, 128), bf),
            pltpu.VMEM((8, SUB, 128), bf),
            pltpu.VMEM((NX, SUB, 512), bf),
            pltpu.VMEM((1024, 2048), bf),
            pltpu.VMEM((NZ, NY, 2, 32, 1024), bf),
            pltpu.VMEM((NZ, NY, 2, 32, 1024), bf),
            pltpu.VMEM((NX, SUB, 2048), bf),
            pltpu.VMEM((3, SUB, 2048), bf),
            pltpu.VMEM((2, SUB, 2048), bf),
            pltpu.VMEM((SUB, 2048), f32),
            pltpu.VMEM((4, SUB // 4, 2048), bf),
            pltpu.VMEM((4, 128, 256), bf),
            pltpu.VMEM((8, 1, 256), f32),
            pltpu.VMEM((1024, 2048), bf),
            dma((160,)),
            dma((12,)),
            dma((8, 2)),
            dma((4, 2)),
            dma((3,)),
            dma((3,)),
            dma((3,)),
            dma((7,)),
            dma((3,)),
            dma((7,)),
            dma((8,)),
            dma((7,)),
            dma((24,)),
            dma((4,)),
            dma((3,)),
            dma((3,)),
            dma((6,)),
            dma((6,)),
            dma((4,)),
            dma((2,)),
        ],
        compiler_params=pltpu.CompilerParams(
            collective_id=0, has_side_effects=True, vmem_limit_bytes=56 * 1024 * 1024
        ),
        cost_estimate=pl.CostEstimate(flops=20_000_000_000, bytes_accessed=4_000_000, transcendentals=17_000_000),
        name="layer",
    )(
        mix_lambda, query_one, query_two, key_one, key_two, values, head_gain.reshape(1, 128), stream, out_weight,
        first_gain.reshape(1, 2048), up_weight, down_weight.T, second_gain.reshape(1, 2048),
    )


def solution(mesh):
    in_specs = (
        P("sp", "tp"), P("sp", "tp"), P("sp", "tp"), P("sp", "tp"), P("sp", "tp"), P("tp"), P(), P("sp", "tp"),
        P("tp", None), P(), P("sp", "tp"), P("tp", "sp"), P(),
    )
    return jax.shard_map(
        local, mesh=mesh, in_specs=in_specs, out_specs=P(("sp", "tp"), None), check_vma=False
    )
```

```python
import functools

import jax
import jax.numpy as jnp
from jax import lax
from jax.experimental import pallas as pl
from jax.experimental.pallas import tpu as pltpu
from jax.sharding import PartitionSpec as P

MESH = pl.DeviceIdType.MESH
NZ, NY, NX = 8, 4, 4
ALPHA = 2.0**0.5
LOG2E = 1.4426950408889634
CEXP = LOG2E * 64 ** (-0.5)
LOW = -1e30
TOK = 256
SUB = 64
NT = (((1,), (1,)), ((), ()))


def layer_norm(value, gain):
    centre = jnp.mean(value, axis=-1, keepdims=True)
    spread = jnp.mean(jnp.square(value - centre), axis=-1, keepdims=True)
    return (value - centre) * lax.rsqrt(spread + 1e-05) * gain


def layer_kernel(
    lam_ref, q1_hbm, q2_hbm, k1_hbm, k2_hbm, v_hbm, hgain_hbm, stream_hbm, ow_hbm, gain1_hbm, up_hbm, down_hbm, gain2_hbm,
    out_ref,
    q1_ref, q2_ref, k1_ref, k2_ref, v_ref, gain_ref, gain1_ref, gain2_ref,
    kvsrc, qsrc, kvbuf, qbuf, acc, mbuf, lbuf, qexp, sbuf, topbuf, osend, ssend, orecv, srecv, attown, attbuf, strbuf,
    wout, wup, wdn, hid, psend, precv, pown, prelay, orelay, srelay, wdnt,
    snd, loc, kv_rcv, q_rcv, o_rcv, s_rcv, str_rcv, att_rcv,
    upy_rcv, upz_rcv, updd_rcv, dnz_rcv, dny_rcv, dndd_rcv, ow_rcv, owdd_rcv, hid_rcv, p_rcv, pr_rcv, or_rcv,
):
    sp = lax.axis_index("sp")
    x = lax.axis_index("tp")
    c = lax.rem(sp, 2)
    y = lax.rem(sp // 2, NY)
    z = sp // (2 * NY)
    f = 1 - 2 * c

    def at_z(d):
        return lax.rem(z + (d + NZ), NZ)

    def at_y(d):
        return lax.rem(y + (d + NY), NY)

    def at_x(d):
        return lax.rem(x + (d + NX), NX)

    def dev(dz=0, dy=0, core=None, dx=0):
        cc = c if core is None else core
        return {"sp": (at_z(dz) * NY + at_y(dy)) * 2 + cc, "tp": at_x(dx)}

    sibling = dev(core=1 - c)
    started = []

    def send(src, dst, rcv, to):
        cp = pltpu.make_async_remote_copy(
            src_ref=src, dst_ref=dst, send_sem=snd.at[len(started)], recv_sem=rcv, device_id=to, device_id_type=MESH
        )
        cp.start()
        started.append(cp)

    def arrived(dst, rcv):
        pltpu.make_async_remote_copy(
            src_ref=dst, dst_ref=dst, send_sem=snd.at[0], recv_sem=rcv, device_id=sibling, device_id_type=MESH
        ).wait_recv()

    mine = pl.ds(pl.multiple_of(x * SUB, SUB), SUB)

    def ow_rows(d, half):
        return pl.ds(pl.multiple_of((2 * at_x(d) + half) * 128, 128), 128)

    local_pairs = [
        (q1_hbm, q1_ref), (q2_hbm, q2_ref), (k1_hbm, k1_ref), (k2_hbm, k2_ref), (v_hbm, v_ref),
        (hgain_hbm, gain_ref), (gain1_hbm, gain1_ref), (gain2_hbm, gain2_ref),
        (stream_hbm.at[mine, :], strbuf.at[x]),
        (up_hbm, wup.at[z, y, c]), (down_hbm, wdn.at[z, y, c]),
        (ow_hbm, wout.at[pl.ds(pl.multiple_of(x * 256, 256), 256), :]),
    ]
    locals_ = [pltpu.make_async_copy(a, b, loc.at[i]) for i, (a, b) in enumerate(local_pairs)]
    for cp in locals_:
        cp.start()

    barrier = pltpu.get_barrier_semaphore()
    partners = [sibling, dev(dy=2)]
    for core in (0, 1):
        partners += [dev(dz=1, core=core), dev(dz=-1, core=core), dev(dy=1, core=core), dev(dy=-1, core=core)]
        partners += [dev(dx=d, core=core) for d in (1, 2, 3)]
    for p in partners:
        pl.semaphore_signal(barrier, inc=1, device_id=p, device_id_type=MESH)

    mbuf[...] = jnp.full(mbuf.shape, LOW, jnp.float32)
    lbuf[...] = jnp.zeros(lbuf.shape, jnp.float32)

    def clear(i, carry):
        acc[i] = jnp.zeros(acc.shape[1:], jnp.float32)
        return carry

    lax.fori_loop(0, acc.shape[0], clear, 0)
    for cp in locals_[:5]:
        cp.wait()

    lane = lax.broadcasted_iota(jnp.int32, (TOK, 128), 1)
    low_half = lane < 64
    q1t = q1_ref[...].astype(jnp.float32).T.astype(jnp.bfloat16)
    q2t = q2_ref[...].astype(jnp.float32).T.astype(jnp.bfloat16)
    for h in (0, 1):
        qsrc[h, 0:64, :] = q1t[64 * h : 64 * h + 64]
        qsrc[h, 64:128, :] = q2t[64 * h : 64 * h + 64]
    vt = v_ref[...].astype(jnp.float32).T.astype(jnp.bfloat16)
    one, two = k1_ref[...].astype(jnp.float32), k2_ref[...].astype(jnp.float32)
    kvsrc[0, 0:256, :] = jnp.where(low_half, one, pltpu.roll(two, 64, 1)).astype(jnp.bfloat16)
    kvsrc[1, 0:256, :] = jnp.where(low_half, pltpu.roll(one, 64, 1), two).astype(jnp.bfloat16)
    for h in (0, 1):
        kvsrc[h, 256:384, :] = vt[128 * h : 128 * h + 128, 0:128]
        kvsrc[h, 384:512, :] = vt[128 * h : 128 * h + 128, 128:256]
    kvbuf[0, c] = kvsrc[c]
    qbuf[0, c] = qsrc[c]
    for i in (9, 10, 11):
        locals_[i].wait()
    pl.semaphore_wait(barrier, len(partners))

    send(qsrc.at[1 - c], qbuf.at[0, c], q_rcv.at[0, c], sibling)
    send(kvsrc.at[1 - c], kvbuf.at[0, c], kv_rcv.at[0, c], sibling)
    for i, d in enumerate((1, -1)):
        send(wdn.at[z, y, c], wdn.at[z, y, c], dnz_rcv.at[i], dev(dz=d))
    for h in (0, 1):
        send(qsrc.at[h], qbuf.at[1, c], q_rcv.at[1, c], dev(dy=1, core=h))
        send(qsrc.at[h], qbuf.at[2, c], q_rcv.at[2, c], dev(dy=-1, core=h))
        send(kvsrc.at[h], kvbuf.at[1, c], kv_rcv.at[1, c], dev(dz=1, core=h))
        send(kvsrc.at[h], kvbuf.at[2, c], kv_rcv.at[2, c], dev(dz=-1, core=h))
    for dx in (1, 2, 3):
        rows = pl.ds(pl.multiple_of(at_x(dx) * SUB, SUB), SUB)
        send(stream_hbm.at[rows, :], strbuf.at[x], str_rcv.at[dx - 1], dev(dx=dx))
    for i, d in enumerate((1, -1)):
        send(wout.at[ow_rows(0, c), :], wout.at[ow_rows(0, c), :], ow_rcv.at[i], dev(dx=d))

    def out_weight_on():
        arrived(wout.at[ow_rows(-1, c), :], ow_rcv.at[0])
        arrived(wout.at[ow_rows(1, c), :], ow_rcv.at[1])
        blk = wout.at[ow_rows(-f, c), :]
        send(blk, blk, ow_rcv.at[2], dev(dx=f))
        for i, d in enumerate((-1, 1)):
            blk = wout.at[ow_rows(d, c), :]
            send(blk, blk, owdd_rcv.at[i], sibling)

    def out_weight_end():
        blk = wout.at[ow_rows(2, c), :]
        arrived(blk, ow_rcv.at[2])
        send(blk, blk, owdd_rcv.at[2], sibling)

    def up_y_start():
        for i, d in enumerate((1, -1)):
            send(wup.at[z, y, c], wup.at[z, y, c], upy_rcv.at[i], dev(dy=d))

    def up_y_on():
        arrived(wup.at[z, at_y(-1), c], upy_rcv.at[0])
        arrived(wup.at[z, at_y(1), c], upy_rcv.at[1])
        blk = wup.at[z, at_y(-f), c]
        send(blk, blk, upy_rcv.at[2], dev(dy=f))

    def up_y_end():
        arrived(wup.at[z, at_y(2), c], upy_rcv.at[2])

    def up_z_start():
        blk = wup.at[z, :, c]
        for i, d in enumerate((1, -1)):
            send(blk, blk, upz_rcv.at[i], dev(dz=d))
        send(blk, blk, updd_rcv.at[0], sibling)

    def up_z_step(d):
        if d == 4:
            blk = wup.at[at_z(4), :, c]
            arrived(blk, upz_rcv.at[6])
            send(blk, blk, updd_rcv.at[7], sibling)
            return
        for i, s in enumerate((-1, 1)):
            blk = wup.at[at_z(s * d), :, c]
            arrived(blk, upz_rcv.at[2 * (d - 1) + i])
            if d < 3:
                send(blk, blk, upz_rcv.at[2 * d + i], dev(dz=-s))
        if d == 3:
            blk = wup.at[at_z(-3 * f), :, c]
            send(blk, blk, upz_rcv.at[6], dev(dz=f))
        for i, s in enumerate((-1, 1)):
            blk = wup.at[at_z(s * d), :, c]
            send(blk, blk, updd_rcv.at[2 * (d - 1) + 1 + i], sibling)

    def down_z_step(d):
        if d == 4:
            arrived(wdn.at[at_z(4), y, c], dnz_rcv.at[6])
            return
        for i, s in enumerate((-1, 1)):
            blk = wdn.at[at_z(s * d), y, c]
            arrived(blk, dnz_rcv.at[2 * (d - 1) + i])
            if d < 3:
                send(blk, blk, dnz_rcv.at[2 * d + i], dev(dz=-s))
        if d == 3:
            blk = wdn.at[at_z(-3 * f), y, c]
            send(blk, blk, dnz_rcv.at[6], dev(dz=f))

    def down_zs(g):
        return {0: ((0, 0),), 1: ((-1, 3), (1, 6)), 2: ((-2, 9), (2, 12)), 3: ((-3, 15), (3, 18)), 4: ((4, 21),)}[g]

    def down_y_start(g):
        for dz, k in down_zs(g):
            blk = wdn.at[at_z(dz), y, c]
            for i, d in enumerate((1, -1)):
                send(blk, blk, dny_rcv.at[k + i], dev(dy=d))

    def down_y_on(g):
        for dz, k in down_zs(g):
            for i, d in enumerate((-1, 1)):
                arrived(wdn.at[at_z(dz), at_y(d), c], dny_rcv.at[k + i])
            blk = wdn.at[at_z(dz), at_y(-f), c]
            send(blk, blk, dny_rcv.at[k + 2], dev(dy=f))

    def down_y_end(g):
        for dz, k in down_zs(g):
            arrived(wdn.at[at_z(dz), at_y(2), c], dny_rcv.at[k + 2])

    def down_over(i):
        blk = wdn.at[:, at_y((0, -1, 1, 2)[i]), c]
        send(blk, blk, dndd_rcv.at[i], sibling)

    def down_here():
        for i, d in enumerate((0, -1, 1, 2)):
            arrived(wdn.at[:, at_y(d), 1 - c], dndd_rcv.at[i])

    def take_kv(slot):
        for cc in (0, 1):
            arrived(kvbuf.at[slot, cc], kv_rcv.at[slot, cc])
            step = 1 if slot % 2 else -1
            if slot <= 4:
                send(kvbuf.at[slot, cc], kvbuf.at[slot + 2, cc], kv_rcv.at[slot + 2, cc], dev(dz=step))
            elif (slot, cc) in ((5, 0), (6, 1)):
                send(kvbuf.at[slot, cc], kvbuf.at[7, cc], kv_rcv.at[7, cc], dev(dz=step))

    def take_q(slot):
        for cc in (0, 1):
            arrived(qbuf.at[slot, cc], q_rcv.at[slot, cc])
            if (slot, cc) in ((1, 0), (2, 1)):
                send(qbuf.at[slot, cc], qbuf.at[3, cc], q_rcv.at[3, cc], dev(dy=1 if slot == 1 else -1))

    def expand(qs):
        for cc in (0, 1):
            scaled = qbuf[qs, cc].astype(jnp.float32) * CEXP
            high = scaled.astype(jnp.bfloat16)
            rest = (scaled - high.astype(jnp.float32)).astype(jnp.bfloat16)
            blank = jnp.zeros((64, 256), jnp.bfloat16)
            for mp in (0, 1):
                own = slice(64 * mp, 64 * mp + 64)
                other = slice(64 - 64 * mp, 128 - 64 * mp)
                at = qs * 4 + 2 * cc + mp
                qexp[at, own, :] = high[own]
                qexp[at, other, :] = blank
                own = slice(128 + 64 * mp, 192 + 64 * mp)
                other = slice(192 - 64 * mp, 256 - 64 * mp)
                qexp[at, own, :] = rest[64 * mp : 64 * mp + 64]
                qexp[at, other, :] = blank

    def score(kvs, qs, j):
        slot = j % 4
        keys = jnp.concatenate([kvbuf[kvs, cc, 0:256, :] for cc in (0, 1)], axis=0)
        keys = jnp.concatenate([keys, keys], axis=1)
        scores = jnp.dot(keys, qexp[qs * 4 + j], preferred_element_type=jnp.float32)
        sbuf[slot] = scores
        topbuf[slot] = jnp.max(scores.reshape(64, 8, 256), axis=0)

    def absorb(kvs, qs, j):
        slot = j % 4
        at = qs * 4 + j
        vals = jnp.concatenate(
            [kvbuf[kvs, cc, 256 + 128 * i : 384 + 128 * i, :] for cc in (0, 1) for i in (0, 1)], axis=1
        )
        old = mbuf[at]
        new = jnp.maximum(old, jnp.max(topbuf[slot], axis=0, keepdims=True))
        factor = jnp.exp2(old - new)
        expo = jnp.exp2(sbuf[slot] - new)
        mbuf[at] = new
        lbuf[at] = lbuf[at] * factor + jnp.sum(expo, axis=0, keepdims=True)
        acc[at] = acc[at] * factor + jnp.dot(vals, expo.astype(jnp.bfloat16), preferred_element_type=jnp.float32)

    def process(kv_lo, kv_n, q_lo, q_n, ready=False, then=None):
        last = kv_n * q_n - 1

        def place(i):
            return kv_lo + i // q_n, q_lo + lax.rem(i, q_n)

        def trip(i, carry):
            kvs, qs = place(i)
            nkvs, nqs = place(jnp.minimum(i + 1, last))
            if then is not None:
                nkvs, nqs = jnp.where(i == last, then[0], nkvs), jnp.where(i == last, then[1], nqs)
            for j in range(4):
                if j < 2:
                    score(kvs, qs, j + 2)
                else:
                    score(nkvs, nqs, j - 2)
                absorb(kvs, qs, j)
            return carry

        if not ready:
            score(kv_lo, q_lo, 0)
            score(kv_lo, q_lo, 1)
        lax.fori_loop(0, last + 1, trip, 0)

    q_direct, q_merged = (3 - f) // 2, (3 + f) // 2

    def finish(qs, place):
        for i in range(4):
            ssend[place, i] = mbuf[qs * 4 + i]
            ssend[place, 4 + i] = lbuf[qs * 4 + i]
        for i in range(4):
            osend[place, i] = (acc[qs * 4 + i] / lbuf[qs * 4 + i]).astype(jnp.bfloat16)

    def opposite_out():
        finish(3, 0)
        send(ssend.at[0], srelay, or_rcv.at[2], dev(dy=f))
        for cc in (0, 1):
            part = pl.ds(2 * cc, 2)
            send(osend.at[0, part], orelay.at[part], or_rcv.at[cc], dev(dy=f))

    def direct_out():
        finish(q_direct, 1)
        send(osend.at[1], orecv.at[0], o_rcv.at[0], dev(dy=-f))
        send(ssend.at[1], srecv.at[0], s_rcv.at[0], dev(dy=-f))

    def merged_out():
        arrived(srelay, or_rcv.at[2])
        shares = []
        for i in range(4):
            m, l = mbuf[q_merged * 4 + i], lbuf[q_merged * 4 + i]
            top = jnp.maximum(m, srelay[i])
            w, v = jnp.exp2(m - top), jnp.exp2(srelay[i] - top) * srelay[4 + i]
            total = l * w + v
            ssend[2, i] = top
            ssend[2, 4 + i] = total
            shares.append((w / total, v / total))
        send(ssend.at[2], srecv.at[1], s_rcv.at[1], dev(dy=f))
        for cc in (0, 1):
            part = pl.ds(2 * cc, 2)
            arrived(orelay.at[part], or_rcv.at[cc])
            for i in (2 * cc, 2 * cc + 1):
                osend[2, i] = (
                    acc[q_merged * 4 + i] * shares[i][0] + orelay[i].astype(jnp.float32) * shares[i][1]
                ).astype(jnp.bfloat16)
            send(osend.at[2, part], orecv.at[1, part], o_rcv.at[1 + cc], dev(dy=f))

    arrived(qbuf.at[0, 1 - c], q_rcv.at[0, 1 - c])
    expand(0)
    arrived(kvbuf.at[0, 1 - c], kv_rcv.at[0, 1 - c])
    process(0, 1, 0, 1)
    down_z_step(1)
    take_q(1)
    take_q(2)
    up_y_start()
    down_y_start(0)
    down_y_start(1)
    expand(1)
    expand(2)
    process(0, 1, 1, 2)
    take_kv(1)
    take_kv(2)
    process(1, 1, 0, 3)
    take_q(3)
    expand(3)
    down_z_step(2)
    down_y_start(2)
    process(0, 2, 3, 1)
    up_y_on()
    down_y_on(0)
    take_kv(3)
    take_kv(4)
    process(2, 1, 0, 4, then=(3, 0))
    down_z_step(3)
    down_y_start(3)
    process(3, 1, 0, 4, ready=True)
    take_kv(5)
    take_kv(6)
    up_y_end()
    up_z_start()
    down_y_on(1)
    down_y_on(2)
    out_weight_on()
    process(4, 1, 0, 4, then=(5, 3))
    process(5, 2, 3, 1, ready=True, then=(5, q_direct))
    down_z_step(4)
    down_y_start(4)
    down_y_on(3)
    down_over(0)
    process(5, 2, q_direct, 1, ready=True)
    take_kv(7)
    process(7, 1, 3, 1, then=(7, q_direct))
    opposite_out()
    process(7, 1, q_direct, 1, ready=True, then=(5, q_merged))
    process(5, 3, q_merged, 1, ready=True, then=(5, 0))
    direct_out()
    out_weight_end()
    process(5, 3, 0, 1, ready=True)
    up_z_step(1)
    merged_out()
    down_y_on(4)

    arrived(orecv.at[0], o_rcv.at[0])
    for j in (0, 1):
        arrived(srecv.at[j], s_rcv.at[j])
    locals_[5].wait()
    lam = lam_ref[c]
    gain = gain_ref[...] * 0.8
    for cc in (0, 1):
        arrived(orecv.at[1, pl.ds(2 * cc, 2)], o_rcv.at[1 + cc])
        maps = []
        for mp in (0, 1):
            i = 2 * cc + mp
            ms = [mbuf[i]] + [srecv[j, i] for j in range(2)]
            ls = [lbuf[i]] + [srecv[j, 4 + i] for j in range(2)]
            top = functools.reduce(jnp.maximum, ms)
            ws = [jnp.exp2(m - top) for m in ms]
            total = ws[0] * ls[0]
            out = acc[i] * ws[0]
            for j in range(2):
                w = ws[j + 1] * ls[j + 1]
                total = total + w
                out = out + orecv[j, i].astype(jnp.float32) * w
            maps.append(out / total)
        mixed = maps[0] - lam * maps[1]
        inv = lax.rsqrt(jnp.mean(mixed * mixed, axis=0, keepdims=True) + 1e-5)
        attown[cc] = ((mixed * inv).T * gain).astype(jnp.bfloat16)


    head = 2 * x + c
    for dx in range(NX):
        for dc in (0, 1):
            if dx == 0 and dc == 0:
                continue
            cc = c if dc == 0 else 1 - c
            rows = pl.ds(pl.multiple_of(at_x(dx) * SUB, SUB), SUB)
            send(attown.at[cc, rows, :], attbuf.at[head], att_rcv.at[2 * dx + dc - 1], dev(dx=dx, core=cc))
    attbuf[head] = attown[c, mine, :]
    up_z_step(2)
    down_over(1)
    down_over(2)
    for i in range(3):
        arrived(wout.at[ow_rows((-1, 1, 2)[i], 1 - c), :], owdd_rcv.at[i])
    for i in (6, 7, 8):
        locals_[i].wait()
    for dx in (1, 2, 3):
        arrived(strbuf.at[at_x(-dx)], str_rcv.at[dx - 1])
    for dx in range(NX):
        for dc in (0, 1):
            if dx == 0 and dc == 0:
                continue
            cc = c if dc == 0 else 1 - c
            arrived(attbuf.at[2 * at_x(-dx) + cc], att_rcv.at[2 * dx + dc - 1])
    attended = jnp.concatenate([attbuf[h] for h in range(8)], axis=1)
    rows = jnp.concatenate([strbuf[i] for i in range(NX)], axis=1).astype(jnp.float32)
    pre = ALPHA * rows + jnp.dot(attended, wout[...], preferred_element_type=jnp.float32)
    own = layer_norm(pre, gain1_ref[...]).astype(jnp.bfloat16)
    hid[x] = own
    halves = [pl.ds(i * (SUB // 2), SUB // 2) for i in (0, 1)]
    for n, half in enumerate(halves):
        send(hid.at[x, half, :], hid.at[x, half, :], hid_rcv.at[n], dev(dx=f))
    for g in range(5):
        down_y_end(g)
    down_over(3)
    up_z_step(3)
    for n, half in enumerate(halves):
        send(hid.at[x, half, :], hid.at[x, half, :], hid_rcv.at[2 + n], dev(dx=-f))
    down_here()
    for i in range(NZ):
        wdnt[:, 256 * i : 256 * i + 256] = wdn[i].reshape(256, 1024).T
    for n, half in enumerate(halves):
        blk = hid.at[at_x(-f), half, :]
        arrived(blk, hid_rcv.at[n])
        send(blk, blk, hid_rcv.at[4 + n], dev(dx=f))
    up_z_step(4)
    arrived(wup.at[z, :, 1 - c], updd_rcv.at[0])
    for d in (1, 2, 3):
        for i, s in enumerate((-1, 1)):
            arrived(wup.at[at_z(s * d), :, 1 - c], updd_rcv.at[2 * (d - 1) + 1 + i])
    arrived(wup.at[at_z(4), :, 1 - c], updd_rcv.at[7])

    def mixer(tokens):
        total = None
        for n in range(4):
            up = wup[:, :, :, :, 256 * n : 256 * n + 256].reshape(2048, 256)
            upper = jnp.dot(tokens, up, preferred_element_type=jnp.float32)
            act = jnp.square(jnp.maximum(upper, 0.0)).astype(jnp.bfloat16)
            part = jnp.dot(act, wdnt[256 * n : 256 * n + 256, :], preferred_element_type=jnp.float32)
            total = part if total is None else total + part
        return total

    post = mixer(own) + ALPHA * own.astype(jnp.float32)
    for n, half in enumerate(halves):
        arrived(hid.at[at_x(f), half, :], hid_rcv.at[2 + n])
    both = mixer(jnp.concatenate([hid[at_x(-f)], hid[at_x(f)]], axis=0))
    psend[0] = both[0:SUB].astype(jnp.bfloat16)
    pown[...] = both[SUB:]
    send(psend.at[0], precv.at[0], p_rcv.at[0], dev(dx=-f))
    for n, half in enumerate(halves):
        arrived(hid.at[at_x(2), half, :], hid_rcv.at[4 + n])
    psend[1] = mixer(hid[at_x(2)]).astype(jnp.bfloat16)
    quarters = [pl.ds(i * (SUB // 4), SUB // 4) for i in range(4)]
    for i, part in enumerate(quarters):
        send(psend.at[1, part, :], prelay.at[i], pr_rcv.at[i], dev(dx=f))
    for i, part in enumerate(quarters):
        arrived(prelay.at[i], pr_rcv.at[i])
        psend[2, part, :] = (pown[part, :] + prelay[i].astype(jnp.float32)).astype(jnp.bfloat16)
        send(psend.at[2, part, :], precv.at[1, part, :], p_rcv.at[1 + i], dev(dx=f))
    arrived(precv.at[0], p_rcv.at[0])
    for i, part in enumerate(quarters):
        arrived(precv.at[1, part, :], p_rcv.at[1 + i])
    for i in range(2):
        post = post + precv[i].astype(jnp.float32)
    out_ref[...] = layer_norm(post, gain2_ref[...]).astype(jnp.bfloat16)
    for cp in started:
        cp.wait_send()


def local(
    query_one, query_two, key_one, key_two, values, mix_lambda, head_gain, stream, out_weight, first_gain,
    up_weight, down_weight, second_gain,
):
    bf, f32 = jnp.bfloat16, jnp.float32
    hbm = pl.BlockSpec(memory_space=pltpu.HBM)
    dma = pltpu.SemaphoreType.DMA
    return pl.pallas_call(
        layer_kernel,
        out_shape=jax.ShapeDtypeStruct((SUB, 2048), bf),
        in_specs=[pl.BlockSpec(memory_space=pltpu.SMEM)] + [hbm] * 12,
        out_specs=pl.BlockSpec(memory_space=pltpu.VMEM),
        scratch_shapes=[
            pltpu.VMEM((256, 128), bf),
            pltpu.VMEM((256, 128), bf),
            pltpu.VMEM((256, 128), bf),
            pltpu.VMEM((256, 128), bf),
            pltpu.VMEM((256, 256), bf),
            pltpu.VMEM((1, 128), f32),
            pltpu.VMEM((1, 2048), f32),
            pltpu.VMEM((1, 2048), f32),
            pltpu.VMEM((2, 512, 128), bf),
            pltpu.VMEM((2, 128, 256), bf),
            pltpu.VMEM((8, 2, 512, 128), bf),
            pltpu.VMEM((4, 2, 128, 256), bf),
            pltpu.VMEM((16, 128, 256), f32),
            pltpu.VMEM((16, 1, 256), f32),
            pltpu.VMEM((16, 1, 256), f32),
            pltpu.VMEM((16, 256, 256), bf),
            pltpu.VMEM((4, 512, 256), f32),
            pltpu.VMEM((4, 8, 256), f32),
            pltpu.VMEM((3, 4, 128, 256), bf),
            pltpu.VMEM((3, 8, 1, 256), f32),
            pltpu.VMEM((2, 4, 128, 256), bf),
            pltpu.VMEM((2, 8, 1, 256), f32),
            pltpu.VMEM((2, 256, 128), bf),
            pltpu.VMEM((8, SUB, 128), bf),
            pltpu.VMEM((NX, SUB, 512), bf),
            pltpu.VMEM((1024, 2048), bf),
            pltpu.VMEM((NZ, NY, 2, 32, 1024), bf),
            pltpu.VMEM((NZ, NY, 2, 32, 1024), bf),
            pltpu.VMEM((NX, SUB, 2048), bf),
            pltpu.VMEM((3, SUB, 2048), bf),
            pltpu.VMEM((2, SUB, 2048), bf),
            pltpu.VMEM((SUB, 2048), f32),
            pltpu.VMEM((4, SUB // 4, 2048), bf),
            pltpu.VMEM((4, 128, 256), bf),
            pltpu.VMEM((8, 1, 256), f32),
            pltpu.VMEM((1024, 2048), bf),
            dma((160,)),
            dma((12,)),
            dma((8, 2)),
            dma((4, 2)),
            dma((3,)),
            dma((3,)),
            dma((3,)),
            dma((7,)),
            dma((3,)),
            dma((7,)),
            dma((8,)),
            dma((7,)),
            dma((24,)),
            dma((4,)),
            dma((3,)),
            dma((3,)),
            dma((6,)),
            dma((6,)),
            dma((4,)),
            dma((3,)),
        ],
        compiler_params=pltpu.CompilerParams(
            collective_id=0, has_side_effects=True, vmem_limit_bytes=56 * 1024 * 1024
        ),
        cost_estimate=pl.CostEstimate(flops=20_000_000_000, bytes_accessed=4_000_000, transcendentals=17_000_000),
        name="layer",
    )(
        mix_lambda, query_one, query_two, key_one, key_two, values, head_gain.reshape(1, 128), stream, out_weight,
        first_gain.reshape(1, 2048), up_weight, down_weight.T, second_gain.reshape(1, 2048),
    )


def solution(mesh):
    in_specs = (
        P("sp", "tp"), P("sp", "tp"), P("sp", "tp"), P("sp", "tp"), P("sp", "tp"), P("tp"), P(), P("sp", "tp"),
        P("tp", None), P(), P("sp", "tp"), P("tp", "sp"), P(),
    )
    return jax.shard_map(
        local, mesh=mesh, in_specs=in_specs, out_specs=P(("sp", "tp"), None), check_vma=False
    )
```

```python
import functools

import jax
import jax.numpy as jnp
from jax import lax
from jax.experimental import pallas as pl
from jax.experimental.pallas import tpu as pltpu
from jax.sharding import PartitionSpec as P

MESH = pl.DeviceIdType.MESH
NZ, NY, NX = 8, 4, 4
ALPHA = 2.0**0.5
LOG2E = 1.4426950408889634
CEXP = LOG2E * 64 ** (-0.5)
LOW = -1e30
TOK = 256
SUB = 64
NT = (((1,), (1,)), ((), ()))


def layer_norm(value, gain):
    centre = jnp.mean(value, axis=-1, keepdims=True)
    spread = jnp.mean(jnp.square(value - centre), axis=-1, keepdims=True)
    return (value - centre) * lax.rsqrt(spread + 1e-05) * gain


def layer_kernel(
    lam_ref, q1_hbm, q2_hbm, k1_hbm, k2_hbm, v_hbm, hgain_hbm, stream_hbm, ow_hbm, gain1_hbm, up_hbm, down_hbm,
    out_ref,
    q1_ref, q2_ref, k1_ref, k2_ref, v_ref, gain_ref, gain1_ref,
    kvsrc, qsrc, kvbuf, qbuf, acc, mbuf, lbuf, qexp, sbuf, topbuf, osend, ssend, orecv, srecv, attown, attbuf, strbuf,
    wout, wup, wdn, hid, psend, precv, pown, prelay, orelay, srelay, wdnt,
    snd, loc, kv_rcv, q_rcv, o_rcv, s_rcv, str_rcv, att_rcv,
    upy_rcv, upz_rcv, updd_rcv, dnz_rcv, dny_rcv, dndd_rcv, ow_rcv, owdd_rcv, hid_rcv, p_rcv, pr_rcv, or_rcv,
):
    sp = lax.axis_index("sp")
    x = lax.axis_index("tp")
    c = lax.rem(sp, 2)
    y = lax.rem(sp // 2, NY)
    z = sp // (2 * NY)
    f = 1 - 2 * c

    def at_z(d):
        return lax.rem(z + (d + NZ), NZ)

    def at_y(d):
        return lax.rem(y + (d + NY), NY)

    def at_x(d):
        return lax.rem(x + (d + NX), NX)

    def dev(dz=0, dy=0, core=None, dx=0):
        cc = c if core is None else core
        return {"sp": (at_z(dz) * NY + at_y(dy)) * 2 + cc, "tp": at_x(dx)}

    sibling = dev(core=1 - c)
    started = []

    def send(src, dst, rcv, to):
        cp = pltpu.make_async_remote_copy(
            src_ref=src, dst_ref=dst, send_sem=snd.at[len(started)], recv_sem=rcv, device_id=to, device_id_type=MESH
        )
        cp.start()
        started.append(cp)

    def arrived(dst, rcv):
        pltpu.make_async_remote_copy(
            src_ref=dst, dst_ref=dst, send_sem=snd.at[0], recv_sem=rcv, device_id=sibling, device_id_type=MESH
        ).wait_recv()

    barrier = pltpu.get_barrier_semaphore()
    partners = [sibling, dev(dy=2)]
    for core in (0, 1):
        partners += [dev(dz=1, core=core), dev(dz=-1, core=core), dev(dy=1, core=core), dev(dy=-1, core=core)]
        partners += [dev(dx=d, core=core) for d in (1, 2, 3)]
    for p in partners:
        pl.semaphore_signal(barrier, inc=1, device_id=p, device_id_type=MESH)

    mine = pl.ds(pl.multiple_of(x * SUB, SUB), SUB)

    def ow_rows(d, half):
        return pl.ds(pl.multiple_of((2 * at_x(d) + half) * 128, 128), 128)

    local_pairs = [
        (q1_hbm, q1_ref), (q2_hbm, q2_ref), (k1_hbm, k1_ref), (k2_hbm, k2_ref), (v_hbm, v_ref),
        (hgain_hbm, gain_ref), (gain1_hbm, gain1_ref),
        (stream_hbm.at[mine, :], strbuf.at[x]),
        (up_hbm, wup.at[z, y, c]), (down_hbm, wdn.at[z, y, c]),
        (ow_hbm, wout.at[pl.ds(pl.multiple_of(x * 256, 256), 256), :]),
    ]
    locals_ = [pltpu.make_async_copy(a, b, loc.at[i]) for i, (a, b) in enumerate(local_pairs)]
    for cp in locals_:
        cp.start()

    for cp in locals_[:5]:
        cp.wait()

    lane = lax.broadcasted_iota(jnp.int32, (TOK, 128), 1)
    low_half = lane < 64
    q1t = q1_ref[...].astype(jnp.float32).T.astype(jnp.bfloat16)
    q2t = q2_ref[...].astype(jnp.float32).T.astype(jnp.bfloat16)
    for h in (0, 1):
        qsrc[h, 0:64, :] = q1t[64 * h : 64 * h + 64]
        qsrc[h, 64:128, :] = q2t[64 * h : 64 * h + 64]
    vt = v_ref[...].astype(jnp.float32).T.astype(jnp.bfloat16)
    one, two = k1_ref[...].astype(jnp.float32), k2_ref[...].astype(jnp.float32)
    kvsrc[0, 0:256, :] = jnp.where(low_half, one, pltpu.roll(two, 64, 1)).astype(jnp.bfloat16)
    kvsrc[1, 0:256, :] = jnp.where(low_half, pltpu.roll(one, 64, 1), two).astype(jnp.bfloat16)
    for h in (0, 1):
        kvsrc[h, 256:384, :] = vt[128 * h : 128 * h + 128, 0:128]
        kvsrc[h, 384:512, :] = vt[128 * h : 128 * h + 128, 128:256]
    kvbuf[0, c] = kvsrc[c]
    qbuf[0, c] = qsrc[c]
    pl.semaphore_wait(barrier, len(partners))

    send(qsrc.at[1 - c], qbuf.at[0, c], q_rcv.at[0, c], sibling)
    send(kvsrc.at[1 - c], kvbuf.at[0, c], kv_rcv.at[0, c], sibling)
    locals_[9].wait()
    for i, d in enumerate((1, -1)):
        send(wdn.at[z, y, c], wdn.at[z, y, c], dnz_rcv.at[i], dev(dz=d))
    for h in (0, 1):
        send(qsrc.at[h], qbuf.at[1, c], q_rcv.at[1, c], dev(dy=1, core=h))
        send(qsrc.at[h], qbuf.at[2, c], q_rcv.at[2, c], dev(dy=-1, core=h))
        send(kvsrc.at[h], kvbuf.at[1, c], kv_rcv.at[1, c], dev(dz=1, core=h))
        send(kvsrc.at[h], kvbuf.at[2, c], kv_rcv.at[2, c], dev(dz=-1, core=h))
    for dx in (1, 2, 3):
        rows = pl.ds(pl.multiple_of(at_x(dx) * SUB, SUB), SUB)
        send(stream_hbm.at[rows, :], strbuf.at[x], str_rcv.at[dx - 1], dev(dx=dx))
    locals_[8].wait()
    locals_[10].wait()
    for i, d in enumerate((1, -1)):
        send(wout.at[ow_rows(0, c), :], wout.at[ow_rows(0, c), :], ow_rcv.at[i], dev(dx=d))

    def out_weight_on():
        arrived(wout.at[ow_rows(-1, c), :], ow_rcv.at[0])
        arrived(wout.at[ow_rows(1, c), :], ow_rcv.at[1])
        blk = wout.at[ow_rows(-f, c), :]
        send(blk, blk, ow_rcv.at[2], dev(dx=f))
        for i, d in enumerate((-1, 1)):
            blk = wout.at[ow_rows(d, c), :]
            send(blk, blk, owdd_rcv.at[i], sibling)

    def out_weight_end():
        blk = wout.at[ow_rows(2, c), :]
        arrived(blk, ow_rcv.at[2])
        send(blk, blk, owdd_rcv.at[2], sibling)

    def up_y_start():
        for i, d in enumerate((1, -1)):
            send(wup.at[z, y, c], wup.at[z, y, c], upy_rcv.at[i], dev(dy=d))

    def up_y_on():
        arrived(wup.at[z, at_y(-1), c], upy_rcv.at[0])
        arrived(wup.at[z, at_y(1), c], upy_rcv.at[1])
        blk = wup.at[z, at_y(-f), c]
        send(blk, blk, upy_rcv.at[2], dev(dy=f))

    def up_y_end():
        arrived(wup.at[z, at_y(2), c], upy_rcv.at[2])

    def up_z_start():
        blk = wup.at[z, :, c]
        for i, d in enumerate((1, -1)):
            send(blk, blk, upz_rcv.at[i], dev(dz=d))
        send(blk, blk, updd_rcv.at[0], sibling)

    def up_z_step(d):
        if d == 4:
            blk = wup.at[at_z(4), :, c]
            arrived(blk, upz_rcv.at[6])
            send(blk, blk, updd_rcv.at[7], sibling)
            return
        for i, s in enumerate((-1, 1)):
            blk = wup.at[at_z(s * d), :, c]
            arrived(blk, upz_rcv.at[2 * (d - 1) + i])
            if d < 3:
                send(blk, blk, upz_rcv.at[2 * d + i], dev(dz=-s))
        if d == 3:
            blk = wup.at[at_z(-3 * f), :, c]
            send(blk, blk, upz_rcv.at[6], dev(dz=f))
        for i, s in enumerate((-1, 1)):
            blk = wup.at[at_z(s * d), :, c]
            send(blk, blk, updd_rcv.at[2 * (d - 1) + 1 + i], sibling)

    def down_z_step(d):
        if d == 4:
            arrived(wdn.at[at_z(4), y, c], dnz_rcv.at[6])
            return
        for i, s in enumerate((-1, 1)):
            blk = wdn.at[at_z(s * d), y, c]
            arrived(blk, dnz_rcv.at[2 * (d - 1) + i])
            if d < 3:
                send(blk, blk, dnz_rcv.at[2 * d + i], dev(dz=-s))
        if d == 3:
            blk = wdn.at[at_z(-3 * f), y, c]
            send(blk, blk, dnz_rcv.at[6], dev(dz=f))

    def down_zs(g):
        return {0: ((0, 0),), 1: ((-1, 3), (1, 6)), 2: ((-2, 9), (2, 12)), 3: ((-3, 15), (3, 18)), 4: ((4, 21),)}[g]

    def down_y_start(g):
        for dz, k in down_zs(g):
            blk = wdn.at[at_z(dz), y, c]
            for i, d in enumerate((1, -1)):
                send(blk, blk, dny_rcv.at[k + i], dev(dy=d))

    def down_y_on(g):
        for dz, k in down_zs(g):
            for i, d in enumerate((-1, 1)):
                arrived(wdn.at[at_z(dz), at_y(d), c], dny_rcv.at[k + i])
            blk = wdn.at[at_z(dz), at_y(-f), c]
            send(blk, blk, dny_rcv.at[k + 2], dev(dy=f))

    def down_y_end(g):
        for dz, k in down_zs(g):
            arrived(wdn.at[at_z(dz), at_y(2), c], dny_rcv.at[k + 2])

    def down_over(i):
        blk = wdn.at[:, at_y((0, -1, 1, 2)[i]), c]
        send(blk, blk, dndd_rcv.at[i], sibling)

    def down_here():
        for i, d in enumerate((0, -1, 1, 2)):
            arrived(wdn.at[:, at_y(d), 1 - c], dndd_rcv.at[i])

    def take_kv(slot):
        for cc in (0, 1):
            arrived(kvbuf.at[slot, cc], kv_rcv.at[slot, cc])
            step = 1 if slot % 2 else -1
            if slot <= 4:
                send(kvbuf.at[slot, cc], kvbuf.at[slot + 2, cc], kv_rcv.at[slot + 2, cc], dev(dz=step))
            elif (slot, cc) in ((5, 0), (6, 1)):
                send(kvbuf.at[slot, cc], kvbuf.at[7, cc], kv_rcv.at[7, cc], dev(dz=step))

    def take_q(slot):
        for cc in (0, 1):
            arrived(qbuf.at[slot, cc], q_rcv.at[slot, cc])
            if (slot, cc) in ((1, 0), (2, 1)):
                send(qbuf.at[slot, cc], qbuf.at[3, cc], q_rcv.at[3, cc], dev(dy=1 if slot == 1 else -1))

    def expand(qs):
        for cc in (0, 1):
            scaled = qbuf[qs, cc].astype(jnp.float32) * CEXP
            high = scaled.astype(jnp.bfloat16)
            rest = (scaled - high.astype(jnp.float32)).astype(jnp.bfloat16)
            blank = jnp.zeros((64, 256), jnp.bfloat16)
            for mp in (0, 1):
                own = slice(64 * mp, 64 * mp + 64)
                other = slice(64 - 64 * mp, 128 - 64 * mp)
                at = qs * 4 + 2 * cc + mp
                qexp[at, own, :] = high[own]
                qexp[at, other, :] = blank
                own = slice(128 + 64 * mp, 192 + 64 * mp)
                other = slice(192 - 64 * mp, 256 - 64 * mp)
                qexp[at, own, :] = rest[64 * mp : 64 * mp + 64]
                qexp[at, other, :] = blank

    def score(kvs, qs, j):
        slot = j % 4
        keys = jnp.concatenate([kvbuf[kvs, cc, 0:256, :] for cc in (0, 1)], axis=0)
        keys = jnp.concatenate([keys, keys], axis=1)
        scores = jnp.dot(keys, qexp[qs * 4 + j], preferred_element_type=jnp.float32)
        sbuf[slot] = scores
        topbuf[slot] = jnp.max(scores.reshape(64, 8, 256), axis=0)

    def absorb(kvs, qs, j):
        slot = j % 4
        at = qs * 4 + j
        vals = jnp.concatenate(
            [kvbuf[kvs, cc, 256 + 128 * i : 384 + 128 * i, :] for cc in (0, 1) for i in (0, 1)], axis=1
        )
        old = mbuf[at]
        new = jnp.maximum(old, jnp.max(topbuf[slot], axis=0, keepdims=True))
        factor = jnp.exp2(old - new)
        expo = jnp.exp2(sbuf[slot] - new)
        mbuf[at] = new
        lbuf[at] = lbuf[at] * factor + jnp.sum(expo, axis=0, keepdims=True)
        acc[at] = acc[at] * factor + jnp.dot(vals, expo.astype(jnp.bfloat16), preferred_element_type=jnp.float32)

    def process(kv_lo, kv_n, q_lo, q_n, ready=False, then=None):
        last = kv_n * q_n - 1

        def place(i):
            return kv_lo + i // q_n, q_lo + lax.rem(i, q_n)

        def trip(i, carry):
            kvs, qs = place(i)
            nkvs, nqs = place(jnp.minimum(i + 1, last))
            if then is not None:
                nkvs, nqs = jnp.where(i == last, then[0], nkvs), jnp.where(i == last, then[1], nqs)
            for j in range(4):
                if j < 2:
                    score(kvs, qs, j + 2)
                else:
                    score(nkvs, nqs, j - 2)
                absorb(kvs, qs, j)
            return carry

        if not ready:
            score(kv_lo, q_lo, 0)
            score(kv_lo, q_lo, 1)
        lax.fori_loop(0, last + 1, trip, 0)

    q_direct, q_merged = (3 - f) // 2, (3 + f) // 2

    def finish(qs, place):
        for i in range(4):
            osend[place, i] = (acc[qs * 4 + i] / lbuf[qs * 4 + i]).astype(jnp.bfloat16)
        for i in range(4):
            ssend[place, i] = mbuf[qs * 4 + i]
            ssend[place, 4 + i] = lbuf[qs * 4 + i]

    def opposite_out():
        finish(3, 0)
        send(osend.at[0], orelay, or_rcv.at[0], dev(dy=f))
        send(ssend.at[0], srelay, or_rcv.at[1], dev(dy=f))

    def direct_out():
        finish(q_direct, 1)
        send(osend.at[1], orecv.at[0], o_rcv.at[0], dev(dy=-f))
        send(ssend.at[1], srecv.at[0], s_rcv.at[0], dev(dy=-f))

    def merged_out():
        arrived(orelay, or_rcv.at[0])
        arrived(srelay, or_rcv.at[1])
        for i in range(4):
            m, l = mbuf[q_merged * 4 + i], lbuf[q_merged * 4 + i]
            top = jnp.maximum(m, srelay[i])
            w, v = jnp.exp2(m - top), jnp.exp2(srelay[i] - top) * srelay[4 + i]
            total = l * w + v
            osend[2, i] = (
                acc[q_merged * 4 + i] * (w / total) + orelay[i].astype(jnp.float32) * (v / total)
            ).astype(jnp.bfloat16)
            ssend[2, i] = top
            ssend[2, 4 + i] = total
        send(osend.at[2], orecv.at[1], o_rcv.at[1], dev(dy=f))
        send(ssend.at[2], srecv.at[1], s_rcv.at[1], dev(dy=f))

    mbuf[...] = jnp.full(mbuf.shape, LOW, jnp.float32)
    lbuf[...] = jnp.zeros(lbuf.shape, jnp.float32)

    def clear(i, carry):
        acc[i] = jnp.zeros(acc.shape[1:], jnp.float32)
        return carry

    lax.fori_loop(0, acc.shape[0], clear, 0)
    arrived(qbuf.at[0, 1 - c], q_rcv.at[0, 1 - c])
    expand(0)
    arrived(kvbuf.at[0, 1 - c], kv_rcv.at[0, 1 - c])
    process(0, 1, 0, 1)
    down_z_step(1)
    take_q(1)
    take_q(2)
    up_y_start()
    down_y_start(0)
    down_y_start(1)
    expand(1)
    expand(2)
    process(0, 1, 1, 2)
    take_kv(1)
    take_kv(2)
    process(1, 1, 0, 3)
    take_q(3)
    expand(3)
    down_z_step(2)
    down_y_start(2)
    process(0, 2, 3, 1)
    take_kv(3)
    take_kv(4)
    up_y_on()
    down_y_on(0)
    process(2, 1, 0, 4, then=(3, 0))
    down_z_step(3)
    down_y_start(3)
    down_y_on(1)
    up_y_end()
    process(3, 1, 0, 4, ready=True)
    take_kv(5)
    take_kv(6)
    up_z_start()
    down_y_on(2)
    out_weight_on()
    process(4, 1, 0, 4, then=(5, 3))
    process(5, 2, 3, 1, ready=True, then=(5, q_direct))
    down_z_step(4)
    down_y_start(4)
    down_y_on(3)
    down_over(0)
    process(5, 2, q_direct, 1, ready=True)
    take_kv(7)
    process(7, 1, 3, 1, then=(7, q_direct))
    opposite_out()
    process(7, 1, q_direct, 1, ready=True, then=(5, q_merged))
    process(5, 3, q_merged, 1, ready=True, then=(5, 0))
    direct_out()
    out_weight_end()
    process(5, 3, 0, 1, ready=True)
    up_z_step(1)
    merged_out()
    down_y_on(4)

    for j in (0, 1):
        arrived(orecv.at[j], o_rcv.at[j])
        arrived(srecv.at[j], s_rcv.at[j])
    locals_[5].wait()
    lam = lam_ref[c]
    gain = gain_ref[...] * 0.8
    for cc in (0, 1):
        maps = []
        for mp in (0, 1):
            i = 2 * cc + mp
            ms = [mbuf[i]] + [srecv[j, i] for j in range(2)]
            ls = [lbuf[i]] + [srecv[j, 4 + i] for j in range(2)]
            top = functools.reduce(jnp.maximum, ms)
            ws = [jnp.exp2(m - top) for m in ms]
            total = ws[0] * ls[0]
            out = acc[i] * ws[0]
            for j in range(2):
                w = ws[j + 1] * ls[j + 1]
                total = total + w
                out = out + orecv[j, i].astype(jnp.float32) * w
            maps.append(out / total)
        mixed = maps[0] - lam * maps[1]
        inv = lax.rsqrt(jnp.mean(mixed * mixed, axis=0, keepdims=True) + 1e-5)
        attown[cc] = ((mixed * inv).T * gain).astype(jnp.bfloat16)


    head = 2 * x + c
    for dx in range(NX):
        for dc in (0, 1):
            if dx == 0 and dc == 0:
                continue
            cc = c if dc == 0 else 1 - c
            rows = pl.ds(pl.multiple_of(at_x(dx) * SUB, SUB), SUB)
            send(attown.at[cc, rows, :], attbuf.at[head], att_rcv.at[2 * dx + dc - 1], dev(dx=dx, core=cc))
    attbuf[head] = attown[c, mine, :]
    up_z_step(2)
    down_over(1)
    down_over(2)
    for i in range(3):
        arrived(wout.at[ow_rows((-1, 1, 2)[i], 1 - c), :], owdd_rcv.at[i])
    for i in (6, 7):
        locals_[i].wait()
    for dx in (1, 2, 3):
        arrived(strbuf.at[at_x(-dx)], str_rcv.at[dx - 1])
    for dx in range(NX):
        for dc in (0, 1):
            if dx == 0 and dc == 0:
                continue
            cc = c if dc == 0 else 1 - c
            arrived(attbuf.at[2 * at_x(-dx) + cc], att_rcv.at[2 * dx + dc - 1])
    attended = jnp.concatenate([attbuf[h] for h in range(8)], axis=1)
    rows = jnp.concatenate([strbuf[i] for i in range(NX)], axis=1).astype(jnp.float32)
    pre = ALPHA * rows + jnp.dot(attended, wout[...], preferred_element_type=jnp.float32)
    own = layer_norm(pre, gain1_ref[...]).astype(jnp.bfloat16)
    hid[x] = own
    halves = [pl.ds(i * (SUB // 2), SUB // 2) for i in (0, 1)]
    for n, half in enumerate(halves):
        send(hid.at[x, half, :], hid.at[x, half, :], hid_rcv.at[n], dev(dx=f))
    for g in range(5):
        down_y_end(g)
    down_over(3)
    up_z_step(3)
    for n, half in enumerate(halves):
        send(hid.at[x, half, :], hid.at[x, half, :], hid_rcv.at[2 + n], dev(dx=-f))
    down_here()
    for i in range(NZ):
        wdnt[:, 256 * i : 256 * i + 256] = wdn[i].reshape(256, 1024).T
    for n, half in enumerate(halves):
        blk = hid.at[at_x(-f), half, :]
        arrived(blk, hid_rcv.at[n])
        send(blk, blk, hid_rcv.at[4 + n], dev(dx=f))
    up_z_step(4)
    arrived(wup.at[z, :, 1 - c], updd_rcv.at[0])
    for d in (1, 2, 3):
        for i, s in enumerate((-1, 1)):
            arrived(wup.at[at_z(s * d), :, 1 - c], updd_rcv.at[2 * (d - 1) + 1 + i])
    arrived(wup.at[at_z(4), :, 1 - c], updd_rcv.at[7])

    def mixer(tokens):
        total = None
        for n in range(4):
            up = wup[:, :, :, :, 256 * n : 256 * n + 256].reshape(2048, 256)
            upper = jnp.dot(tokens, up, preferred_element_type=jnp.float32)
            act = jnp.square(jnp.maximum(upper, 0.0)).astype(jnp.bfloat16)
            part = jnp.dot(act, wdnt[256 * n : 256 * n + 256, :], preferred_element_type=jnp.float32)
            total = part if total is None else total + part
        return total

    post = mixer(own) + ALPHA * own.astype(jnp.float32)
    for n, half in enumerate(halves):
        arrived(hid.at[at_x(f), half, :], hid_rcv.at[2 + n])
    both = mixer(jnp.concatenate([hid[at_x(-f)], hid[at_x(f)]], axis=0))
    psend[0] = both[0:SUB].astype(jnp.bfloat16)
    pown[...] = both[SUB:]
    send(psend.at[0], precv.at[0], p_rcv.at[0], dev(dx=-f))
    for n, half in enumerate(halves):
        arrived(hid.at[at_x(2), half, :], hid_rcv.at[4 + n])
    psend[1] = mixer(hid[at_x(2)]).astype(jnp.bfloat16)
    quarters = [pl.ds(i * (SUB // 4), SUB // 4) for i in range(4)]
    for i, part in enumerate(quarters):
        send(psend.at[1, part, :], prelay.at[i], pr_rcv.at[i], dev(dx=f))
    for i, part in enumerate(quarters):
        arrived(prelay.at[i], pr_rcv.at[i])
        psend[2, part, :] = (pown[part, :] + prelay[i].astype(jnp.float32)).astype(jnp.bfloat16)
        send(psend.at[2, part, :], precv.at[1, part, :], p_rcv.at[1 + i], dev(dx=f))
    arrived(precv.at[0], p_rcv.at[0])
    for i, part in enumerate(quarters):
        arrived(precv.at[1, part, :], p_rcv.at[1 + i])
    for i in range(2):
        post = post + precv[i].astype(jnp.float32)
    out_ref[...] = layer_norm(post, 1.0)
    for cp in started:
        cp.wait_send()


def local(
    query_one, query_two, key_one, key_two, values, mix_lambda, head_gain, stream, out_weight, first_gain,
    up_weight, down_weight, second_gain,
):
    bf, f32 = jnp.bfloat16, jnp.float32
    hbm = pl.BlockSpec(memory_space=pltpu.HBM)
    dma = pltpu.SemaphoreType.DMA
    normed = pl.pallas_call(
        layer_kernel,
        out_shape=jax.ShapeDtypeStruct((SUB, 2048), f32),
        in_specs=[pl.BlockSpec(memory_space=pltpu.SMEM)] + [hbm] * 11,
        out_specs=pl.BlockSpec(memory_space=pltpu.VMEM),
        scratch_shapes=[
            pltpu.VMEM((256, 128), bf),
            pltpu.VMEM((256, 128), bf),
            pltpu.VMEM((256, 128), bf),
            pltpu.VMEM((256, 128), bf),
            pltpu.VMEM((256, 256), bf),
            pltpu.VMEM((1, 128), f32),
            pltpu.VMEM((1, 2048), f32),
            pltpu.VMEM((2, 512, 128), bf),
            pltpu.VMEM((2, 128, 256), bf),
            pltpu.VMEM((8, 2, 512, 128), bf),
            pltpu.VMEM((4, 2, 128, 256), bf),
            pltpu.VMEM((16, 128, 256), f32),
            pltpu.VMEM((16, 1, 256), f32),
            pltpu.VMEM((16, 1, 256), f32),
            pltpu.VMEM((16, 256, 256), bf),
            pltpu.VMEM((4, 512, 256), f32),
            pltpu.VMEM((4, 8, 256), f32),
            pltpu.VMEM((3, 4, 128, 256), bf),
            pltpu.VMEM((3, 8, 1, 256), f32),
            pltpu.VMEM((2, 4, 128, 256), bf),
            pltpu.VMEM((2, 8, 1, 256), f32),
            pltpu.VMEM((2, 256, 128), bf),
            pltpu.VMEM((8, SUB, 128), bf),
            pltpu.VMEM((NX, SUB, 512), bf),
            pltpu.VMEM((1024, 2048), bf),
            pltpu.VMEM((NZ, NY, 2, 32, 1024), bf),
            pltpu.VMEM((NZ, NY, 2, 32, 1024), bf),
            pltpu.VMEM((NX, SUB, 2048), bf),
            pltpu.VMEM((3, SUB, 2048), bf),
            pltpu.VMEM((2, SUB, 2048), bf),
            pltpu.VMEM((SUB, 2048), f32),
            pltpu.VMEM((4, SUB // 4, 2048), bf),
            pltpu.VMEM((4, 128, 256), bf),
            pltpu.VMEM((8, 1, 256), f32),
            pltpu.VMEM((1024, 2048), bf),
            dma((160,)),
            dma((12,)),
            dma((8, 2)),
            dma((4, 2)),
            dma((3,)),
            dma((3,)),
            dma((3,)),
            dma((7,)),
            dma((3,)),
            dma((7,)),
            dma((8,)),
            dma((7,)),
            dma((24,)),
            dma((4,)),
            dma((3,)),
            dma((3,)),
            dma((6,)),
            dma((6,)),
            dma((4,)),
            dma((2,)),
        ],
        compiler_params=pltpu.CompilerParams(
            collective_id=0, has_side_effects=True, vmem_limit_bytes=56 * 1024 * 1024
        ),
        cost_estimate=pl.CostEstimate(flops=20_000_000_000, bytes_accessed=4_000_000, transcendentals=17_000_000),
        name="layer",
    )(
        mix_lambda, query_one, query_two, key_one, key_two, values, head_gain.reshape(1, 128), stream, out_weight,
        first_gain.reshape(1, 2048), up_weight, down_weight.T,
    )
    return (normed * second_gain).astype(bf)


def solution(mesh):
    in_specs = (
        P("sp", "tp"), P("sp", "tp"), P("sp", "tp"), P("sp", "tp"), P("sp", "tp"), P("tp"), P(), P("sp", "tp"),
        P("tp", None), P(), P("sp", "tp"), P("tp", "sp"), P(),
    )
    return jax.shard_map(
        local, mesh=mesh, in_specs=in_specs, out_specs=P(("sp", "tp"), None), check_vma=False
    )
```
